32 devices in a mesh: sp: 8 (over z, y), tp: 4 (over x, core).
Axes of the slice: x: 2, y: 2, z: 4, core: 2. Of those that a mesh axis runs over, the one named last changes fastest.
Arguments:
- resid: bfloat16 [6144, 2048], P(('sp', 'tp')), may hold values from -6 to 6
- query_small: bfloat16 [6144, 768], P('sp', 'tp'), may hold values from -480 to 480
- query_large: bfloat16 [6144, 1280], P('sp', 'tp'), may hold values from -480 to 480
- kv_latent: bfloat16 [6144, 256], P('sp'), may hold values from -6 to 6
- rope_key: bfloat16 [6144, 32], P('sp'), may hold values from -6 to 6
- kv_gain: bfloat16 [256], replicated, may hold values from 0.099609375 to 1.8984375
- up_key_small: bfloat16 [256, 512], P(None, 'tp'), may hold values from -0.375 to 0.375
- up_value_small: bfloat16 [256, 512], P(None, 'tp'), may hold values from -0.375 to 0.375
- up_key_large: bfloat16 [256, 1024], P(None, 'tp'), may hold values from -0.375 to 0.375
- up_value_large: bfloat16 [256, 1024], P(None, 'tp'), may hold values from -0.375 to 0.375
- out_weight: bfloat16 [1536, 2048], replicated, may hold values from -0.359375 to 0.359375
- mix_gain: bfloat16 [2048], replicated, may hold values from 0.099609375 to 1.8984375
- gate_weight: bfloat16 [2048, 5632], P('sp', 'tp'), may hold values from -0.125 to 0.125
- up_weight: bfloat16 [2048, 5632], P('sp', 'tp'), may hold values from -0.125 to 0.125
- down_weight: bfloat16 [2048, 5632], P('sp', 'tp'), may hold values from -0.078125 to 0.078125
Outputs:
- layer_output: bfloat16 [6144, 2048], P(('sp', 'tp'))
The draws below stay inside these ranges and needn't reach their ends.
All inputs are finite; a program needn't handle non-finite values.
Results may differ from the reference program's by a relative error of at most 0.014.
The reference program's roundings to bfloat16 on the way count: a program that leaves them out, or rounds other values in their place, can miss the bound.
Values may be sent and summed in bfloat16 or wider, within the bound.
A program may use at most 128 MiB of HBM per device.

```python
import math
import jax
import jax.numpy as jnp
from jax import lax

D = 2048
HEADS_SMALL = 8
HEADS_LARGE = 8
NOPE_SMALL = 64
NOPE_LARGE = 128
VALUE_SMALL = 64
VALUE_LARGE = 128
ROTARY = 32
LATENT = 256
FF = 5632
TOK_DEV = 768
SEQ = 6144
N_TP = 4


def drawn_query(key, columns):
    base = 2.0 * jax.random.truncated_normal(key, -6.0, 6.0, (SEQ, columns), jnp.float32)
    return base


def draw_query_small(key, part):
    return drawn_query(jax.random.fold_in(key, 11), HEADS_SMALL * (NOPE_SMALL + ROTARY)).astype(jnp.bfloat16)


def draw_query_large(key, part):
    return drawn_query(jax.random.fold_in(key, 13), HEADS_LARGE * (NOPE_LARGE + ROTARY)).astype(jnp.bfloat16)


def steps_of(key, shape, split, low, high):
    loudness = 1.0
    for dim, shards_of in split:
        steps = jax.random.uniform(jax.random.fold_in(jax.random.fold_in(key, 6), dim), (shards_of,), jnp.float32, low / len(split), high / len(split))
        loudness = loudness * jnp.repeat(jnp.exp(steps), shape[dim] // shards_of).reshape((-1,) + (1,) * (len(shape) - 1 - dim))
    return loudness


def normal_values(own_key, extent, scale, bound, shards=(), held_as=jnp.bfloat16):
    factor_of = steps_of(own_key, extent, shards, -0.22, 0.18) if shards else 1.0
    drawn = jax.random.normal(own_key, extent, jnp.float32) * scale * factor_of
    return jnp.minimum(jnp.maximum(drawn, -bound), bound).astype(held_as)


def setup_inputs(seed: int = 0) -> dict:
    arg_keys = jax.random.split(jax.random.key(seed), 16)
    return {
        "resid": normal_values(arg_keys[0], (SEQ, D), 1.0, 6.0, ((0, 32),)),
        "query_small": draw_query_small(jax.random.fold_in(arg_keys[15], 71), 0),
        "query_large": draw_query_large(jax.random.fold_in(arg_keys[15], 71), 0),
        "kv_latent": normal_values(arg_keys[3], (SEQ, LATENT), 1.0, 6.0, ((0, 8),)),
        "rope_key": normal_values(arg_keys[4], (SEQ, ROTARY), 1.0, 6.0, ((0, 8),)),
        "kv_gain": jnp.clip(1.0 + 0.18 * jax.random.normal(arg_keys[5], (LATENT,), jnp.float32), 0.099609375, 1.8984375).astype(jnp.bfloat16),
        "up_key_small": normal_values(arg_keys[6], (LATENT, HEADS_SMALL * NOPE_SMALL), LATENT ** -0.5, 0.375, ((1, 4),)),
        "up_value_small": normal_values(arg_keys[7], (LATENT, HEADS_SMALL * VALUE_SMALL), LATENT ** -0.5, 0.375, ((1, 4),)),
        "up_key_large": normal_values(arg_keys[8], (LATENT, HEADS_LARGE * NOPE_LARGE), LATENT ** -0.5, 0.375, ((1, 4),)),
        "up_value_large": normal_values(arg_keys[9], (LATENT, HEADS_LARGE * VALUE_LARGE), LATENT ** -0.5, 0.375, ((1, 4),)),
        "out_weight": normal_values(arg_keys[10], (HEADS_SMALL * VALUE_SMALL + HEADS_LARGE * VALUE_LARGE, D), 0.06, 0.359375),
        "mix_gain": jnp.clip(1.0 + 0.18 * jax.random.normal(arg_keys[11], (D,), jnp.float32), 0.099609375, 1.8984375).astype(jnp.bfloat16),
        "gate_weight": normal_values(arg_keys[12], (D, FF), D ** -0.5, 0.125, ((0, 8), (1, 4))),
        "up_weight": normal_values(arg_keys[13], (D, FF), D ** -0.5, 0.125, ((0, 8), (1, 4))),
        "down_weight": normal_values(arg_keys[14], (D, FF), FF ** -0.5, 0.078125, ((0, 8), (1, 4))),
    }


THETA = 10000.0
EPSILON = 1e-06
FLOOR = -1e+30

def angles(positions, width):
    inverse = THETA ** (-jnp.arange(0, width, 2).astype(jnp.float32) / width)
    phase = positions.astype(jnp.float32)[:, None] * inverse[None, :]
    return (jnp.cos(phase), jnp.sin(phase))

def rotate(values, angle_cos, angle_sin):
    half = values.shape[-1] // 2
    first = values[..., :half].astype(jnp.float32)
    second = values[..., half:].astype(jnp.float32)
    turned = jnp.concatenate([first * angle_cos - second * angle_sin, second * angle_cos + first * angle_sin], axis=-1)
    return turned.astype(jnp.bfloat16)

def norm_rows(values, gain):
    wide = values.astype(jnp.float32)
    scaled = wide * lax.rsqrt(lax.optimization_barrier(jnp.mean(wide * wide, axis=-1, keepdims=True)) + EPSILON)
    return (scaled * gain.astype(jnp.float32)).astype(jnp.bfloat16)

def attend(query, key_nope, shared_key, values, nope):
    length = query.shape[0]
    heads = query.shape[1]
    scale = 1.0 / math.sqrt(nope + shared_key.shape[1])
    count = length // TOK_DEV
    key_wide = key_nope.astype(jnp.float32)
    shared_wide = shared_key.astype(jnp.float32)
    value_wide = values.astype(jnp.float32)

    def one_block(index):
        start = index * TOK_DEV
        block = lax.dynamic_slice_in_dim(query, start, TOK_DEV, 0).astype(jnp.float32)
        scores = jnp.einsum('qhd,khd->hqk', block[..., :nope], key_wide)
        scores = scores + jnp.einsum('qhd,kd->hqk', block[..., nope:], shared_wide)
        scores = scores * scale
        query_pos = start + jnp.arange(TOK_DEV).astype(jnp.int32)
        key_pos = jnp.arange(length).astype(jnp.int32)
        allowed = key_pos[None, :] <= query_pos[:, None]
        scores = jnp.where(allowed[None], scores, FLOOR)
        maximum = lax.optimization_barrier(jnp.max(scores, axis=-1, keepdims=True))
        weights = jnp.where(allowed[None], jnp.exp(scores - maximum), 0.0)
        total = lax.optimization_barrier(jnp.sum(weights, axis=-1))
        rounded = lax.optimization_barrier(weights.astype(jnp.bfloat16)).astype(jnp.float32)
        summed = jnp.einsum('hqk,khd->qhd', rounded, value_wide)
        return (summed / jnp.transpose(total)[:, :, None]).astype(jnp.bfloat16)
    out = lax.map(one_block, jnp.arange(count).astype(jnp.int32))
    return out.reshape(length, -1)

def reference(resid, query_small, query_large, kv_latent, rope_key, kv_gain, up_key_small, up_value_small, up_key_large, up_value_large, out_weight, mix_gain, gate_weight, up_weight, down_weight):
    length = kv_latent.shape[0]
    positions = jnp.arange(length).astype(jnp.int32)
    angle_cos, angle_sin = angles(positions, ROTARY)
    latent_normed = norm_rows(kv_latent, kv_gain)
    rotated_key = rotate(rope_key, angle_cos, angle_sin)

    def group(query, up_key, up_value, heads, nope, width):
        shaped = query.reshape(length, heads, nope + ROTARY)
        turned = rotate(shaped[..., nope:], angle_cos[:, None, :], angle_sin[:, None, :])
        full_query = jnp.concatenate([shaped[..., :nope], turned], axis=-1)
        keys = jnp.dot(latent_normed, up_key, preferred_element_type=jnp.float32).astype(jnp.bfloat16)
        values = jnp.dot(latent_normed, up_value, preferred_element_type=jnp.float32).astype(jnp.bfloat16)
        return attend(full_query, keys.reshape(length, heads, nope), rotated_key, values.reshape(length, heads, width), nope)
    attn_small = group(query_small, up_key_small, up_value_small, HEADS_SMALL, NOPE_SMALL, VALUE_SMALL)
    attn_large = group(query_large, up_key_large, up_value_large, HEADS_LARGE, NOPE_LARGE, VALUE_LARGE)
    border = HEADS_SMALL * VALUE_SMALL
    mixed = jnp.dot(attn_small, out_weight[:border], preferred_element_type=jnp.float32)
    mixed = mixed + jnp.dot(attn_large, out_weight[border:], preferred_element_type=jnp.float32)
    middle = (resid.astype(jnp.float32) + mixed).astype(jnp.bfloat16)
    middle_wide = lax.optimization_barrier(middle).astype(jnp.float32)
    mixer_in = norm_rows(middle, mix_gain)
    gate = jnp.dot(mixer_in, gate_weight, preferred_element_type=jnp.float32)
    upward = jnp.dot(mixer_in, up_weight, preferred_element_type=jnp.float32)
    hidden = (jax.nn.silu(gate) * upward).astype(jnp.bfloat16)
    width = FF // N_TP
    total = middle_wide
    for index in range(N_TP):
        part = jnp.dot(hidden[:, index * width:(index + 1) * width], jnp.transpose(down_weight[:, index * width:(index + 1) * width]), preferred_element_type=jnp.float32).astype(jnp.bfloat16)
        total = total + lax.optimization_barrier(part).astype(jnp.float32)
    return total.astype(jnp.bfloat16)
```

```python
import functools
import math

import jax
import jax.numpy as jnp
from jax import lax
from jax.experimental import pallas as pl
from jax.experimental.pallas import tpu as pltpu
from jax.sharding import PartitionSpec as P

HEADS_SMALL = 8
NOPE_SMALL = 64
NOPE_LARGE = 128
VALUE_SMALL = 64
VALUE_LARGE = 128
ROTARY = 32


THETA = 10000.0
EPSILON = 1e-06
FLOOR = -1e30


def angles(positions, width):
    inverse = THETA ** (-jnp.arange(0, width, 2).astype(jnp.float32) / width)
    phase = positions.astype(jnp.float32)[:, None] * inverse[None, :]
    return (jnp.cos(phase), jnp.sin(phase))


def rotate(values, angle_cos, angle_sin):
    half = values.shape[-1] // 2
    first = values[..., :half].astype(jnp.float32)
    second = values[..., half:].astype(jnp.float32)
    turned = jnp.concatenate(
        [first * angle_cos - second * angle_sin, second * angle_cos + first * angle_sin], axis=-1
    )
    return turned.astype(jnp.bfloat16)


def norm_rows(values, gain):
    wide = values.astype(jnp.float32)
    scaled = wide * lax.rsqrt(jnp.mean(wide * wide, axis=-1, keepdims=True) + EPSILON)
    return (scaled * gain.astype(jnp.float32)).astype(jnp.bfloat16)


LOG2E = math.log2(math.e)
TILE = 256
PAD = 16


def layer(count, owners, passes, *refs):
    (kv_own, expand_key, expand_value, resid, gain, out_weight) = refs[:6]
    weights = refs[6:9]
    queries = refs[9:11]
    result = refs[11]
    (kv, whole, arrived_a, arrived_b, outs_a, outs_b, joined, projection, resid_all, middle) = refs[12:22]
    (mixer, gated, parts, kept, maxima, sums) = refs[22:28]
    (kv_recv, kv_up, kv_y, kv_d, w_recv, w_z, w_zr, w_y, w_d, own_sem) = refs[28:38]
    (r_send, r_recv, a_send, a_recv, m_send, m_recv, p_send, p_recv) = refs[38:]
    arrived, outs = (arrived_a, arrived_b), (outs_a, outs_b)

    deep = 1 << ((count.bit_length() - 1) // 2)
    tall = count // deep
    pairs = owners // 2
    blocks = count - 1
    me = lax.axis_index("sp")
    col = lax.axis_index("tp")
    z, y = lax.div(me, deep), lax.rem(me, deep)
    x, core = lax.div(col, 2), lax.rem(col, 2)
    odd = lax.rem(z, 2)
    prime = core == odd
    other = z + 1 - 2 * odd
    token = (z - odd + core) * deep + y
    group = x * 2 + odd
    twin = x * 2 + 1 - core
    rows = kv_own.shape[0]
    depth, hidden = weights[0].shape
    mine = resid.shape[0]
    width = resid.shape[1]
    half = rows // 2

    def send(source, target, out_sem, in_sem, sp, tp):
        return pltpu.make_async_remote_copy(
            src_ref=source,
            dst_ref=target,
            send_sem=out_sem,
            recv_sem=in_sem,
            device_id={"sp": sp, "tp": tp},
            device_id_type=pl.DeviceIdType.MESH,
        )

    barrier = pltpu.get_barrier_semaphore()

    def greet(sp, tp):
        pl.semaphore_signal(
            barrier, inc=1, device_id={"sp": sp, "tp": tp}, device_id_type=pl.DeviceIdType.MESH
        )

    for ahead in range(1, tall):
        greet(lax.rem(z + ahead, tall) * deep + y, col)
    for ahead in range(1, deep):
        greet(z * deep + lax.rem(y + ahead, deep), col)
    for ahead in range(1, owners):
        greet(me, lax.rem(col + ahead, owners))
        greet(other * deep + y, lax.rem(col + ahead, owners))
    pl.semaphore_wait(barrier, tall - 1 + deep - 1 + 2 * (owners - 1))

    def kv_at(src, part):
        return kv.at[pl.ds(pl.multiple_of(src * rows + part * half, half), half)]

    def own_half():
        return kv_own.at[pl.ds(pl.multiple_of(core * half, half), half)]

    def latent_up(src, away):
        source = own_half() if src is None else kv_at(src, core)
        block = me if src is None else src
        return send(source, kv_at(block, core), kv_up.at[away], kv_recv.at[block, core], me + deep, col)

    def latent_over(src, away, ahead):
        source = own_half() if src is None else kv_at(src, core)
        block = me if src is None else src
        to = z * deep + lax.rem(y + ahead, deep)
        return send(source, kv_at(block, core), kv_y.at[away, ahead - 1], kv_recv.at[block, core], to, col)

    def latent_twin(src, step):
        return send(kv_at(src, core), kv_at(src, core), kv_d.at[step], kv_recv.at[src, core], me, twin)

    def latent_wait(src, part):
        send(kv_at(src, part), kv_at(src, part), kv_d.at[0], kv_recv.at[src, part], me, twin).wait_recv()

    latent_keep = pltpu.make_async_copy(
        kv_own, kv.at[pl.ds(pl.multiple_of(me * rows, rows), rows)], own_sem.at[3]
    )
    latent_keep.start()

    @pl.when(z + 1 < tall)
    def _():
        latent_up(None, 0).start()

    for ahead in range(1, deep):

        @pl.when(y + ahead < deep)
        def _():
            latent_over(None, 0, ahead).start()

    def latent_step(step):
        src = me - step
        away = z - lax.div(src, deep)
        latent_wait(src, core)

        @pl.when(lax.rem(src, deep) == y)
        def _():
            @pl.when(z + 1 < tall)
            def _():
                latent_up(src, away).start()

            for ahead in range(1, deep):
                latent_over(src, away, ahead).start()

        latent_twin(src, step).start()
        latent_wait(src, 1 - core)

    def listed(place):
        return jnp.where(z < tall // 2, lax.rem(z + place, tall), lax.rem(z - place + tall, tall))

    def slab(which, src):
        return whole.at[which, pl.ds(pl.multiple_of(src * depth, depth), depth)]

    def weight_z(source, which, src, sem, to):
        return send(source, slab(which, src), sem, w_recv.at[which, src], to * deep + y, col)

    def weight_y(source, which, src, sem, ahead):
        to = z * deep + lax.rem(y + ahead, deep)
        return send(source, slab(which, src), sem, w_recv.at[which, src], to, col)

    def weight_twin(source, which, src, sem):
        return send(source, slab(which, src), sem, w_recv.at[which, src], me, twin)

    def weight_wait(which, src):
        weight_twin(slab(which, src), which, src, w_d.at[which, 0]).wait_recv()

    stride = jnp.where(prime, 2, 1)

    def own_sends(which):
        source = weights[which]

        @pl.when(z + stride < tall)
        def _():
            weight_z(source, which, me, w_z.at[which, 0], z + stride).start()

        @pl.when(z - stride >= 0)
        def _():
            weight_z(source, which, me, w_z.at[which, 1], z - stride).start()

        @pl.when(prime)
        def _():
            for ahead in range(1, deep):
                weight_y(source, which, me, w_y.at[which, 0, ahead - 1], ahead).start()
            weight_twin(source, which, me, w_d.at[which, 0]).start()
            pltpu.make_async_copy(source, slab(which, me), own_sem.at[which]).start()

    def place_of(index):
        turn, spot = lax.div(index, deep), lax.rem(index, deep)
        final = turn == tall - 1
        straight = (spot == 0) & (turn < tall - 1)
        place = jnp.where(straight, turn + 1, turn)
        over = jnp.where(straight, 0, jnp.where(final, spot + 1, spot))
        zs = listed(place)
        return straight, place, zs, zs * deep + lax.rem(y + over, deep)

    def relay(which, index):
        straight, place, zs, src = place_of(index)
        weight_wait(which, src)
        block = slab(which, src)

        @pl.when(straight)
        def _():
            @pl.when((zs < z) & (z + 2 < tall))
            def _():
                weight_z(block, which, src, w_zr.at[which, place], z + 2).start()

            @pl.when((zs > z) & (z - 2 >= 0))
            def _():
                weight_z(block, which, src, w_zr.at[which, place], z - 2).start()

            for ahead in range(1, deep):
                weight_y(block, which, src, w_y.at[which, place, ahead - 1], ahead).start()

        weight_twin(block, which, src, w_d.at[which, index + 1]).start()

    def event(number):
        for which, early, late in ((1, 2, 3), (2, blocks + 2, 5)):

            @pl.when(number == jnp.where(prime, early, late))
            def _():
                own_sends(which)

        @pl.when(prime & (number < 3 * blocks))
        def _():
            relay(lax.div(number, blocks), lax.rem(number, blocks))

    def targets():
        for far in range(2):
            for ahead in range(pairs):
                block = me if far == 0 else other * deep + y
                yield far, ahead, block, lax.rem(x + ahead, pairs) * 2 + odd

    def share(far, ahead, copy):
        if far == 0 and ahead == 0:

            @pl.when(jnp.logical_not(prime))
            def _():
                copy()
        else:
            copy()

    def resid_send(far, ahead, sp, tp):
        return send(resid, resid_all.at[pl.ds(pl.multiple_of(col * mine, mine), mine)],
                    r_send.at[far, ahead], r_recv.at[col], sp, tp)

    def attn_send(number, far, ahead, sp, tp):
        return send(outs[number], arrived[number].at[col],
                    a_send.at[number, far, ahead], a_recv.at[number, col], sp, tp)

    own_sends(0)
    for far, ahead, sp, tp in targets():
        share(far, ahead, lambda: resid_send(far, ahead, sp, tp).start())
    resid_keep = pltpu.make_async_copy(
        resid, resid_all.at[pl.ds(pl.multiple_of(col * mine, mine), mine)], own_sem.at[4]
    )

    @pl.when(prime)
    def _():
        resid_keep.start()

    projection_keep = pltpu.make_async_copy(out_weight, projection, own_sem.at[5])
    projection_keep.start()
    latent_keep.wait()

    def tiles(number, index, diagonal):
        start = pl.multiple_of(index * rows, rows)
        latent = kv[pl.ds(start, rows), :]
        for head, (inner, nope, wide, key_at, size, value_at, sum_at) in enumerate(passes[number]):
            key = jnp.dot(
                latent, expand_key[:, key_at : key_at + wide], preferred_element_type=jnp.float32
            ).astype(jnp.bfloat16)
            value = lax.dot_general(
                expand_value[value_at : value_at + size, :],
                latent[:, : expand_value.shape[1]],
                (((1,), (1,)), ((), ())),
                preferred_element_type=jnp.float32,
            ).astype(jnp.bfloat16)
            value = jnp.concatenate([value, jnp.ones((PAD, rows), jnp.bfloat16)], axis=0)
            scale = LOG2E / math.sqrt(nope + ROTARY)
            for tile in range(rows // TILE):
                columns = slice(tile * TILE, (tile + 1) * TILE)
                length = (tile + 1) * TILE if diagonal else rows
                scores = jnp.dot(
                    key[:length], queries[number][inner, :, columns], preferred_element_type=jnp.float32
                )
                place = slice(sum_at, sum_at + size + PAD)
                if diagonal:
                    key_pos = lax.broadcasted_iota(jnp.int32, scores.shape, 0)
                    query_pos = lax.broadcasted_iota(jnp.int32, scores.shape, 1) + tile * TILE
                    scores = jnp.where(key_pos <= query_pos, scores, FLOOR)
                    new = jnp.max(scores, axis=0, keepdims=True)
                    weight = jnp.exp2((scores - new) * scale).astype(jnp.bfloat16)
                    maxima[head, :, columns] = new
                    sums[place, columns] = jnp.dot(
                        value[:, :length], weight, preferred_element_type=jnp.float32
                    )
                else:
                    old = maxima[head, :, columns]
                    new = jnp.maximum(old, jnp.max(scores, axis=0, keepdims=True))
                    weight = jnp.exp2((scores - new) * scale).astype(jnp.bfloat16)
                    factor = jnp.exp2((old - new) * scale)
                    maxima[head, :, columns] = new
                    sums[place, columns] = sums[place, columns] * factor + jnp.dot(
                        value, weight, preferred_element_type=jnp.float32
                    )

    def finish(number):
        for inner, nope, wide, key_at, size, value_at, sum_at in passes[number]:
            for tile in range(rows // TILE):
                columns = slice(tile * TILE, (tile + 1) * TILE)
                total = sums[sum_at : sum_at + size, columns] / sums[sum_at + size : sum_at + size + 1, columns]
                outs[number][columns, inner * size : (inner + 1) * size] = total.T.astype(jnp.bfloat16)
        for far, ahead, sp, tp in targets():
            share(far, ahead, lambda: attn_send(number, far, ahead, sp, tp).start())

        @pl.when(prime)
        def _():
            arrived[number][col] = outs[number][...]

    tiles(0, me, True)

    def first_step(step, carry):
        latent_step(step)
        event(step - 1)
        tiles(0, me - step, False)
        return carry

    lax.fori_loop(1, me + 1, first_step, 0)
    finish(0)
    tiles(1, me, True)

    def second_step(step, carry):
        @pl.when(lax.rem(step, 2) == 1)
        def _():
            event(me + lax.div(step, 2))

        tiles(1, me - step, False)
        return carry

    lax.fori_loop(1, me + 1, second_step, 0)
    finish(1)
    done = me + lax.div(me + 1, 2)

    def drain(first, last):
        lax.fori_loop(first, last, lambda number, carry: (event(number), carry)[1], 0)
        return jnp.maximum(first, last)

    done = drain(done, blocks)
    for far, ahead, sp, tp in targets():
        share(far, ahead, lambda: resid_send(far, ahead, sp, tp).wait_send())
        for number in range(2):
            share(far, ahead, lambda: attn_send(number, far, ahead, sp, tp).wait_send())

    @pl.when(prime)
    def _():
        resid_keep.wait()

    projection_keep.wait()
    for tp in range(owners):

        @pl.when(jnp.logical_not(prime) | (tp != col))
        def _():
            send(resid, resid_all.at[pl.ds(tp * mine, mine)], r_send.at[0, 0], r_recv.at[tp], me, twin).wait_recv()
            for number in range(2):
                send(outs[number], arrived[number].at[tp], a_send.at[number, 0, 0],
                     a_recv.at[number, tp], me, twin).wait_recv()

        size_a, size_b = outs[0].shape[1], outs[1].shape[1]
        large_from = owners * size_b
        joined[:, tp * size_b : (tp + 1) * size_b] = arrived[1][tp]
        joined[:, large_from + tp * size_a : large_from + (tp + 1) * size_a] = arrived[0][tp]

    features = projection.shape[0]

    def project(part, squares):
        at = pl.ds(pl.multiple_of(part * TILE, TILE), TILE)
        mixed = jnp.dot(joined[:, :features], projection[:, at], preferred_element_type=jnp.float32)
        rounded = (resid_all[:, at].astype(jnp.float32) + mixed).astype(jnp.bfloat16)
        middle[:, at] = rounded
        wide = rounded.astype(jnp.float32)
        return squares + jnp.sum(wide * wide, axis=1, keepdims=True)

    squares = lax.fori_loop(0, width // TILE, project, jnp.zeros((rows, 1), jnp.float32))
    scaling = lax.rsqrt(squares * (1.0 / width) + EPSILON)

    def normalise(part, carry):
        at = pl.ds(pl.multiple_of(part * TILE, TILE), TILE)
        scaled = middle[:, at].astype(jnp.float32) * scaling
        mixer[:, at] = (scaled * gain[:, at].astype(jnp.float32)).astype(jnp.bfloat16)
        return carry

    lax.fori_loop(0, width // TILE, normalise, 0)

    def share_middle():
        at = pl.ds(pl.multiple_of(twin * mine, mine), mine)
        return send(middle.at[at], kept, m_send, m_recv, me, twin)

    @pl.when(prime)
    def _():
        share_middle().start()
        kept[...] = middle[pl.ds(pl.multiple_of(col * mine, mine), mine), :]

    def ready(which, first):
        last = drain(first, (which + 1) * blocks)

        @pl.when(prime)
        def _():
            pltpu.make_async_copy(weights[which], slab(which, me), own_sem.at[which]).wait()

        @pl.when(jnp.logical_not(prime))
        def _():
            lax.fori_loop(0, count, lambda src, carry: (weight_wait(which, src), carry)[1], 0)

        return last

    spans = hidden // TILE

    def over_hidden(body):
        def step(part, carry):
            body(pl.ds(pl.multiple_of(part * TILE, TILE), TILE))
            return carry

        lax.fori_loop(0, spans, step, 0)
        if hidden % TILE:
            body(pl.ds(spans * TILE, hidden % TILE))

    done = ready(0, done)

    def gate_part(at):
        gated[:, at] = jnp.dot(mixer[...], whole[0, :, at], preferred_element_type=jnp.float32)

    over_hidden(gate_part)
    done = ready(1, done)

    def up_part(at):
        value = jnp.dot(mixer[...], whole[1, :, at], preferred_element_type=jnp.float32)
        opened = gated[:, at]
        joined[:, at] = (opened / (1.0 + jnp.exp(-opened)) * value).astype(jnp.bfloat16)

    over_hidden(up_part)
    done = drain(done, 2 * blocks)

    def part_send(block, tp):
        at = pl.ds(pl.multiple_of(block * depth, depth), depth)
        return send(resid_all.at[pl.ds(tp * mine, mine), at], parts.at[group, :, at],
                    p_send.at[tp], p_recv.at[group], token, tp)

    def lower(turn, carry):
        src = jnp.where(turn == 0, me, place_of(jnp.maximum(turn - 1, 0))[3])

        @pl.when(prime & (turn == 0))
        def _():
            pltpu.make_async_copy(weights[2], slab(2, me), own_sem.at[2]).wait()

        @pl.when(prime & (2 * blocks + turn > done))
        def _():
            event(2 * blocks + turn - 1)

        @pl.when(jnp.logical_not(prime))
        def _():
            weight_wait(2, src)

        at = pl.ds(pl.multiple_of(src * depth, depth), depth)
        partial = lax.dot_general(
            joined[:, :hidden], whole[2, at, :], (((1,), (1,)), ((), ())),
            preferred_element_type=jnp.float32,
        ).astype(jnp.bfloat16)
        resid_all[:, at] = partial
        for tp in range(owners):
            local = prime & (tp == col)

            @pl.when(jnp.logical_not(local))
            def _():
                part_send(src, tp).start()

            @pl.when(local)
            def _():
                parts[group, :, at] = resid_all[tp * mine : (tp + 1) * mine, at]

        return carry

    lax.fori_loop(0, count, lower, 0)

    for tp in range(owners):
        local = prime & (tp == col)

        @pl.when(jnp.logical_not(local))
        def _():
            whole_part = parts.at[tp]
            send(resid_all.at[pl.ds(tp * mine, mine)], whole_part, p_send.at[tp], p_recv.at[tp], me, twin).wait_send()
            send(resid_all.at[pl.ds(tp * mine, mine)], whole_part, p_send.at[tp], p_recv.at[tp], me, twin).wait_recv()

    @pl.when(prime)
    def _():
        share_middle().wait_send()

    @pl.when(jnp.logical_not(prime))
    def _():
        share_middle().wait_recv()

    total = kept[...].astype(jnp.float32)
    for tp in range(owners):
        total = total + parts[tp].astype(jnp.float32)
    result[...] = total.astype(jnp.bfloat16)

    @pl.when(z + 1 < tall)
    def _():
        latent_up(None, 0).wait_send()

    for ahead in range(1, deep):

        @pl.when(y + ahead < deep)
        def _():
            latent_over(None, 0, ahead).wait_send()

    def latent_close(step, carry):
        src = me - step
        away = z - lax.div(src, deep)

        @pl.when(lax.rem(src, deep) == y)
        def _():
            @pl.when(z + 1 < tall)
            def _():
                latent_up(src, away).wait_send()

            for ahead in range(1, deep):
                latent_over(src, away, ahead).wait_send()

        latent_twin(src, step).wait_send()
        return carry

    lax.fori_loop(1, me + 1, latent_close, 0)

    def weight_close(which, carry):
        @pl.when(z + stride < tall)
        def _():
            weight_z(slab(which, me), which, me, w_z.at[which, 0], z + stride).wait_send()

        @pl.when(z - stride >= 0)
        def _():
            weight_z(slab(which, me), which, me, w_z.at[which, 1], z - stride).wait_send()

        @pl.when(prime)
        def _():
            for place in range(tall):
                zs = listed(place)

                @pl.when(((zs < z) & (z + 2 < tall)) | ((zs > z) & (z - 2 >= 0)))
                def _():
                    weight_z(slab(which, me), which, me, w_zr.at[which, place], z).wait_send()

                for ahead in range(1, deep):
                    weight_y(slab(which, me), which, me, w_y.at[which, place, ahead - 1], ahead).wait_send()

            for index in range(count):
                weight_twin(slab(which, me), which, me, w_d.at[which, index]).wait_send()

        return carry

    lax.fori_loop(0, 3, weight_close, 0)


def on_device(
    count,
    owners,
    resid,
    query_small,
    query_large,
    kv_latent,
    rope_key,
    kv_gain,
    up_key_small,
    up_value_small,
    up_key_large,
    up_value_large,
    out_weight,
    mix_gain,
    gate_weight,
    up_weight,
    down_weight,
):
    rows, latent_size = kv_latent.shape
    mine, width = resid.shape
    offset = lax.axis_index("sp") * rows
    positions = offset + jnp.arange(rows, dtype=jnp.int32)
    angle_cos, angle_sin = angles(positions, ROTARY)
    held = -(-(latent_size + ROTARY) // 128) * 128
    spare = held - latent_size - ROTARY
    shared = jnp.concatenate(
        [
            norm_rows(kv_latent, kv_gain),
            rotate(rope_key, angle_cos, angle_sin),
            jnp.zeros((rows, spare), jnp.bfloat16),
        ],
        axis=1,
    )

    passes = []
    queries, keys, values = [], [], []
    key_at = value_at = 0
    for query, up_key, up_value, nope, size in (
        (query_large, up_key_large, up_value_large, NOPE_LARGE, VALUE_LARGE),
        (query_small, up_key_small, up_value_small, NOPE_SMALL, VALUE_SMALL),
    ):
        heads = up_key.shape[1] // nope
        wide = nope + ROTARY
        padded = -(-wide // 128) * 128
        shaped = query.reshape(rows, heads, wide)
        turned = rotate(shaped[..., nope:], angle_cos[:, None, :], angle_sin[:, None, :])
        full = jnp.concatenate([shaped[..., :nope], turned], axis=-1)
        full = jnp.pad(full, ((0, 0), (0, 0), (0, padded - wide)))
        queries.append(jnp.transpose(full, (1, 2, 0)))
        rotary_part = jnp.eye(ROTARY, padded, k=nope, dtype=jnp.bfloat16)
        group = []
        for head in range(heads):
            part = jnp.pad(up_key[:, head * nope : (head + 1) * nope], ((0, 0), (0, padded - nope)))
            blank = jnp.zeros((spare, padded), jnp.bfloat16)
            keys.append(jnp.concatenate([part, rotary_part, blank], axis=0))
            group.append((head, nope, padded, key_at, size, value_at, head * (size + PAD)))
            key_at += padded
            value_at += size
        passes.append(tuple(group))
        values.append(jnp.transpose(up_value))
    expand_key = jnp.concatenate(keys, axis=1)
    expand_value = jnp.concatenate(values, axis=0)
    depth, hidden = gate_weight.shape
    features = out_weight.shape[0]
    sizes = [len(group) * group[0][4] for group in passes]
    most = max(len(group) for group in passes)
    tallest = max(len(group) * (group[0][4] + PAD) for group in passes)
    deep = 1 << ((count.bit_length() - 1) // 2)
    tall = count // deep
    pairs = owners // 2
    vmem = pl.BlockSpec(memory_space=pltpu.VMEM)
    hbm = pl.BlockSpec(memory_space=pl.ANY)
    bf16, f32 = jnp.bfloat16, jnp.float32
    dma = pltpu.SemaphoreType.DMA
    return pl.pallas_call(
        functools.partial(layer, count, owners, tuple(passes)),
        out_shape=jax.ShapeDtypeStruct((mine, width), bf16),
        in_specs=[hbm, vmem, vmem, hbm, vmem, hbm, hbm, hbm, hbm, vmem, vmem],
        out_specs=vmem,
        scratch_shapes=[
            pltpu.VMEM((count * rows, held), bf16),
            pltpu.VMEM((3, count * depth, hidden), bf16),
            pltpu.VMEM((owners, rows, sizes[0]), bf16),
            pltpu.VMEM((owners, rows, sizes[1]), bf16),
            pltpu.VMEM((rows, sizes[0]), bf16),
            pltpu.VMEM((rows, sizes[1]), bf16),
            pltpu.VMEM((rows, max(features, hidden)), bf16),
            pltpu.VMEM((features, width), bf16),
            pltpu.VMEM((owners * mine, width), bf16),
            pltpu.VMEM((rows, width), bf16),
            pltpu.VMEM((rows, width), bf16),
            pltpu.VMEM((rows, hidden), f32),
            pltpu.VMEM((owners, mine, width), bf16),
            pltpu.VMEM((mine, width), bf16),
            pltpu.VMEM((most, 1, rows), f32),
            pltpu.VMEM((tallest, rows), f32),
            dma((count, 2)),
            dma((tall,)),
            dma((tall, deep)),
            dma((count,)),
            dma((3, count)),
            dma((3, 2)),
            dma((3, tall)),
            dma((3, tall, deep)),
            dma((3, count)),
            dma((6,)),
            dma((2, pairs)),
            dma((owners,)),
            dma((2, 2, pairs)),
            dma((2, owners)),
            dma,
            dma,
            dma((owners,)),
            dma((owners,)),
        ],
        compiler_params=pltpu.CompilerParams(
            collective_id=0, has_side_effects=True, vmem_limit_bytes=67043328
        ),
        cost_estimate=pl.CostEstimate(
            flops=10**11, bytes_accessed=3 * 10**7, transcendentals=2 * 10**7
        ),
    )(
        shared,
        expand_key,
        expand_value,
        resid,
        mix_gain.reshape(1, width),
        out_weight,
        gate_weight,
        up_weight,
        down_weight,
        queries[0],
        queries[1],
    )


def solution(mesh):
    placed = (
        P(("sp", "tp"), None),
        P("sp", "tp"),
        P("sp", "tp"),
        P("sp", None),
        P("sp", None),
        P(),
        P(None, "tp"),
        P(None, "tp"),
        P(None, "tp"),
        P(None, "tp"),
        P(),
        P(),
        P("sp", "tp"),
        P("sp", "tp"),
        P("sp", "tp"),
    )
    return jax.shard_map(
        functools.partial(on_device, mesh.shape["sp"], mesh.shape["tp"]), mesh=mesh, in_specs=placed, out_specs=P(("sp", "tp"), None), check_vma=False
    )
```

```python
import functools
import math

import jax
import jax.numpy as jnp
from jax import lax
from jax.experimental import pallas as pl
from jax.experimental.pallas import tpu as pltpu
from jax.sharding import PartitionSpec as P

HEADS_SMALL = 8
NOPE_SMALL = 64
NOPE_LARGE = 128
VALUE_SMALL = 64
VALUE_LARGE = 128
ROTARY = 32


THETA = 10000.0
EPSILON = 1e-06
FLOOR = -1e30


def angles(positions, width):
    inverse = THETA ** (-jnp.arange(0, width, 2).astype(jnp.float32) / width)
    phase = positions.astype(jnp.float32)[:, None] * inverse[None, :]
    return (jnp.cos(phase), jnp.sin(phase))


def rotate(values, angle_cos, angle_sin):
    half = values.shape[-1] // 2
    first = values[..., :half].astype(jnp.float32)
    second = values[..., half:].astype(jnp.float32)
    turned = jnp.concatenate(
        [first * angle_cos - second * angle_sin, second * angle_cos + first * angle_sin], axis=-1
    )
    return turned.astype(jnp.bfloat16)


def norm_rows(values, gain):
    wide = values.astype(jnp.float32)
    scaled = wide * lax.rsqrt(jnp.mean(wide * wide, axis=-1, keepdims=True) + EPSILON)
    return (scaled * gain.astype(jnp.float32)).astype(jnp.bfloat16)


LOG2E = math.log2(math.e)
TILE = 256
PAD = 16
LANES = 128
SPIN = NOPE_SMALL


def layer(count, owners, passes, *refs):
    (kv_own, expand_key, expand_value, resid, gain, out_weight) = refs[:6]
    weights = refs[6:9]
    queries = refs[9:11]
    result = refs[11]
    (kv, turned, whole, arrived_a, arrived_b, outs_a, outs_b, joined, projection, resid_all, middle) = refs[12:23]
    (mixer, gated, parts, kept, maxima, sums) = refs[23:29]
    (kv_recv, kv_up, kv_y, kv_d, w_recv, w_z, w_zr, w_y, w_d, own_sem) = refs[29:39]
    (r_send, r_recv, r_pass, a_send, a_recv, a_pass, s_send, s_recv) = refs[39:47]
    (m_send, m_recv, p_send, p_recv, halves) = refs[47:]
    arrived, outs = (arrived_a, arrived_b), (outs_a, outs_b)

    deep = 1 << ((count.bit_length() - 1) // 2)
    tall = count // deep
    pairs = owners // 2
    blocks = count - 1
    me = lax.axis_index("sp")
    col = lax.axis_index("tp")
    z, y = lax.div(me, deep), lax.rem(me, deep)
    x, core = lax.div(col, 2), lax.rem(col, 2)
    odd = lax.rem(z, 2)
    prime = core == odd
    other = z + 1 - 2 * odd
    token = (z - odd + core) * deep + y
    group = x * 2 + odd
    twin = x * 2 + 1 - core
    rows = queries[0].shape[2]
    depth, hidden = weights[0].shape
    mine = resid.shape[0]
    width = resid.shape[1]
    half = rows // 2

    def send(source, target, out_sem, in_sem, sp, tp):
        return pltpu.make_async_remote_copy(
            src_ref=source,
            dst_ref=target,
            send_sem=out_sem,
            recv_sem=in_sem,
            device_id={"sp": sp, "tp": tp},
            device_id_type=pl.DeviceIdType.MESH,
        )

    barrier = pltpu.get_barrier_semaphore()

    def greet(sp, tp):
        pl.semaphore_signal(
            barrier, inc=1, device_id={"sp": sp, "tp": tp}, device_id_type=pl.DeviceIdType.MESH
        )

    for ahead in range(1, tall):
        greet(lax.rem(z + ahead, tall) * deep + y, col)
    for ahead in range(1, deep):
        greet(z * deep + lax.rem(y + ahead, deep), col)
    for ahead in range(1, owners):
        greet(me, lax.rem(col + ahead, owners))
        greet(other * deep + y, lax.rem(col + ahead, owners))
    greet(lax.rem(z - 1 + 2 * odd + tall, tall) * deep + y, twin)
    pl.semaphore_wait(barrier, tall - 1 + deep - 1 + 2 * (owners - 1) + 1)

    def latent_up(source, src, away):
        lead = x * 2 + 1 - odd
        return send(source, kv.at[src], kv_up.at[away], kv_recv.at[src], me + deep, lead)

    def latent_over(source, src, away, ahead):
        to = z * deep + lax.rem(y + ahead, deep)
        return send(source, kv.at[src], kv_y.at[away, ahead - 1], kv_recv.at[src], to, col)

    def latent_twin(src):
        return send(kv.at[src], kv.at[src], kv_d.at[src], kv_recv.at[src], me, twin)

    def latent_own(act):
        @pl.when(prime & (z + 1 < tall))
        def _():
            act(latent_up(kv_own, me, 0))

        for ahead in range(1, deep):

            @pl.when(jnp.logical_not(prime) & (y + ahead < deep))
            def _():
                act(latent_over(kv_own, me, 0, ahead))

    def latent_row(away, act):
        src = me - away * deep

        @pl.when(prime)
        def _():
            @pl.when(z + 1 < tall)
            def _():
                act(latent_up(kv.at[src], src, away))

            act(latent_twin(src))

        @pl.when(jnp.logical_not(prime))
        def _():
            for ahead in range(1, deep):
                act(latent_over(kv.at[src], src, away, ahead))

    def latent_source(step):
        rest = jnp.maximum(step - y - 1, 0)
        spot = lax.rem(rest, deep)
        near = step <= y
        level = jnp.where(near, 0, 1 + lax.div(rest, deep))
        over = jnp.where(near, y - step, lax.rem(y + spot, deep))
        return (z - level) * deep + over, jnp.logical_not(near) & (spot == 0)

    latent_keep = pltpu.make_async_copy(kv_own, kv.at[me], own_sem.at[3])
    latent_keep.start()
    latent_own(lambda copy: copy.start())

    def latent_step(step):
        @pl.when(step <= z)
        def _():
            latent_twin(me - step * deep).wait_recv()
            latent_row(step, lambda copy: copy.start())

        src, straight = latent_source(step)

        @pl.when(jnp.logical_not(straight))
        def _():
            latent_twin(src).wait_recv()

            @pl.when(jnp.logical_not(prime))
            def _():
                latent_twin(src).start()

    def listed(place):
        rising = jnp.where(place - 1 < z, place - 1, place)
        falling = jnp.where(tall - place > z, tall - place, tall - 1 - place)
        return jnp.where(place == 0, z, jnp.where(z < tall // 2, rising, falling))

    def slab(which, src):
        return whole.at[which, pl.ds(pl.multiple_of(src * depth, depth), depth)]

    def weight_z(source, which, src, sem, to):
        return send(source, slab(which, src), sem, w_recv.at[which, src], to * deep + y, col)

    def weight_y(source, which, src, sem, ahead):
        to = z * deep + lax.rem(y + ahead, deep)
        return send(source, slab(which, src), sem, w_recv.at[which, src], to, col)

    def weight_twin(source, which, src, sem):
        return send(source, slab(which, src), sem, w_recv.at[which, src], me, twin)

    def weight_wait(which, src):
        weight_twin(slab(which, src), which, src, w_d.at[which, 0]).wait_recv()

    stride = jnp.where(prime, 2, 1)

    def own_up(which):
        @pl.when(z + stride < tall)
        def _():
            weight_z(weights[which], which, me, w_z.at[which, 0], z + stride).start()

    def own_down(which):
        @pl.when(z - stride >= 0)
        def _():
            weight_z(weights[which], which, me, w_z.at[which, 1], z - stride).start()

    def own_over(which):
        source = weights[which]

        @pl.when(prime)
        def _():
            for ahead in range(1, deep):
                weight_y(source, which, me, w_y.at[which, 0, ahead - 1], ahead).start()
            weight_twin(source, which, me, w_d.at[which, 0]).start()
            pltpu.make_async_copy(source, slab(which, me), own_sem.at[which]).start()

    def place_of(index):
        turn, spot = lax.div(index, deep), lax.rem(index, deep)
        final = turn == tall - 1
        straight = (spot == 0) & (turn < tall - 1)
        place = jnp.where(straight, turn + 1, turn)
        over = jnp.where(straight, 0, jnp.where(final, spot + 1, spot))
        zs = listed(place)
        return straight, place, zs, zs * deep + lax.rem(y + over, deep)

    def relay(which, index):
        straight, place, zs, src = place_of(index)
        weight_wait(which, src)
        block = slab(which, src)

        @pl.when(straight)
        def _():
            @pl.when((zs < z) & (z + 2 < tall))
            def _():
                weight_z(block, which, src, w_zr.at[which, place], z + 2).start()

            @pl.when((zs > z) & (z - 2 >= 0))
            def _():
                weight_z(block, which, src, w_zr.at[which, place], z - 2).start()

            for ahead in range(1, deep):
                weight_y(block, which, src, w_y.at[which, place, ahead - 1], ahead).start()

        weight_twin(block, which, src, w_d.at[which, index + 1]).start()

    def event(number):
        @pl.when(prime & (number == 1))
        def _():
            own_up(1)

        @pl.when(prime & (number == 4))
        def _():
            own_over(2)

        @pl.when(prime & (number == blocks))
        def _():
            own_up(2)

        @pl.when(prime & (number < 3 * blocks))
        def _():
            relay(lax.div(number, blocks), lax.rem(number, blocks))

    def targets():
        for far in range(2):
            for ahead in range(pairs):
                block = me if far == 0 else other * deep + y
                yield far, ahead, block, lax.rem(x + ahead, pairs) * 2 + odd

    def share(far, ahead, copy):
        if far == 0 and ahead == 0:

            @pl.when(jnp.logical_not(prime))
            def _():
                copy()
        else:
            copy()

    def resid_at(tp):
        return resid_all.at[pl.ds(pl.multiple_of(tp * mine, mine), mine)]

    def resid_sends(act):
        for far, ahead, sp, tp in targets():
            if far == 0 or ahead == 0:
                share(far, ahead, lambda: act(
                    send(resid, resid_at(col), r_send.at[far, ahead], r_recv.at[col], sp, tp)))

    def resid_passes(act, wait):
        for side in range(2):
            source = x * 2 + side
            block = resid_at(source)
            if wait:
                send(block, block, r_pass.at[side, 0], r_recv.at[source], me, twin).wait_recv()
            for ahead in range(1, pairs):
                act(send(block, block, r_pass.at[side, ahead], r_recv.at[source],
                         me, lax.rem(x + ahead, pairs) * 2 + core))

    def attn_sends(number, act):
        for far, ahead, sp, tp in targets():
            if far == 0 or ahead == 0:
                share(far, ahead, lambda: act(
                    send(outs[number], arrived[number].at[col], a_send.at[number, far, ahead],
                         a_recv.at[number, col], sp, tp)))

    def attn_passes(number, act, wait):
        for side in range(2):
            source = x * 2 + side
            block = arrived[number].at[source]
            if wait:
                send(block, block, a_pass.at[number, side, 0], a_recv.at[number, source], me, twin).wait_recv()
            for ahead in range(1, pairs):
                act(send(block, block, a_pass.at[number, side, ahead], a_recv.at[number, source],
                         me, lax.rem(x + ahead, pairs) * 2 + core))

    def early_up():
        own_up(0)

        @pl.when(odd == 0)
        def _():
            resid_sends(lambda copy: copy.start())

    own_down(0)
    own_over(0)
    pl.when(jnp.logical_not(prime) & (z > 0))(early_up)

    @pl.when(odd == 1)
    def _():
        resid_sends(lambda copy: copy.start())

    @pl.when(jnp.logical_not(prime))
    def _():
        own_down(1)

        @pl.when(odd == 0)
        def _():
            own_down(2)

    def first_up():
        pl.when(prime | (z == 0))(early_up)

        @pl.when(jnp.logical_not(prime))
        def _():
            own_up(1)

            @pl.when(odd == 1)
            def _():
                own_up(2)

    resid_keep = pltpu.make_async_copy(
        resid, resid_all.at[pl.ds(pl.multiple_of(col * mine, mine), mine)], own_sem.at[4]
    )

    @pl.when(prime)
    def _():
        resid_keep.start()

    projection_keep = pltpu.make_async_copy(out_weight, projection, own_sem.at[5])
    projection_keep.start()
    latent_keep.wait()

    def unpack(index):
        for part in range(2):
            packed = kv[index, part, half:]
            thick = packed.shape[0]
            for piece in range(half // thick):
                slim = packed[:, piece * ROTARY : (piece + 1) * ROTARY]
                before = jnp.zeros((thick, SPIN), jnp.bfloat16)
                after = jnp.zeros((thick, LANES - SPIN - ROTARY), jnp.bfloat16)
                turned[pl.ds(pl.multiple_of(index * rows + part * half + piece * thick, thick), thick), :] = (
                    jnp.concatenate([before, slim, after], axis=1)
                )

    def tiles(number, index, diagonal):
        latent = jnp.concatenate([kv[index, 0, :half], kv[index, 1, :half]], axis=0)
        spun = turned[pl.ds(pl.multiple_of(index * rows, rows), rows), :]
        for head, (inner, nope, wide, key_at, size, value_at, sum_at) in enumerate(passes[number]):
            key = jnp.dot(
                latent, expand_key[:, key_at : key_at + wide], preferred_element_type=jnp.float32
            ).astype(jnp.bfloat16)
            key = jnp.concatenate([key, spun], axis=1) if nope % LANES == 0 else key + spun
            value = lax.dot_general(
                expand_value[value_at : value_at + size, :],
                latent,
                (((1,), (1,)), ((), ())),
                preferred_element_type=jnp.float32,
            ).astype(jnp.bfloat16)
            value = jnp.concatenate([value, jnp.ones((PAD, rows), jnp.bfloat16)], axis=0)
            scale = LOG2E / math.sqrt(nope + ROTARY)
            for tile in range(rows // TILE):
                columns = slice(tile * TILE, (tile + 1) * TILE)
                length = (tile + 1) * TILE if diagonal else rows
                scores = jnp.dot(
                    key[:length], queries[number][inner, :, columns], preferred_element_type=jnp.float32
                )
                place = slice(sum_at, sum_at + size + PAD)
                if diagonal:
                    key_pos = lax.broadcasted_iota(jnp.int32, scores.shape, 0)
                    query_pos = lax.broadcasted_iota(jnp.int32, scores.shape, 1) + tile * TILE
                    scores = jnp.where(key_pos <= query_pos, scores, FLOOR)
                    new = jnp.max(scores, axis=0, keepdims=True)
                    weight = jnp.exp2((scores - new) * scale).astype(jnp.bfloat16)
                    maxima[head, :, columns] = new
                    sums[place, columns] = jnp.dot(
                        value[:, :length], weight, preferred_element_type=jnp.float32
                    )
                else:
                    old = maxima[head, :, columns]
                    new = jnp.maximum(old, jnp.max(scores, axis=0, keepdims=True))
                    weight = jnp.exp2((scores - new) * scale).astype(jnp.bfloat16)
                    factor = jnp.exp2((old - new) * scale)
                    maxima[head, :, columns] = new
                    sums[place, columns] = sums[place, columns] * factor + jnp.dot(
                        value, weight, preferred_element_type=jnp.float32
                    )

    def finish(number):
        for inner, nope, wide, key_at, size, value_at, sum_at in passes[number]:
            for tile in range(rows // TILE):
                columns = slice(tile * TILE, (tile + 1) * TILE)
                total = sums[sum_at : sum_at + size, columns] / sums[sum_at + size : sum_at + size + 1, columns]
                outs[number][columns, inner * size : (inner + 1) * size] = total.T.astype(jnp.bfloat16)
        attn_sends(number, lambda copy: copy.start())

        @pl.when(prime)
        def _():
            arrived[number][col] = outs[number][...]

    unpack(me)
    tiles(0, me, True)

    def first_step(step, carry):
        latent_step(step)

        @pl.when(prime & (step == jnp.minimum(me, 3)))
        def _():
            own_down(1)

        src, straight = latent_source(step)
        unpack(src)
        tiles(0, src, False)
        return carry

    lax.fori_loop(1, me + 1, first_step, 0)
    finish(0)

    first_up()
    own_over(1)
    tiles(1, me, True)

    def second_step(step, carry):
        @pl.when(step > 2)
        def _():
            event(step - 3)

        tiles(1, me - step, False)
        return carry

    lax.fori_loop(1, me + 1, second_step, 0)
    finish(1)

    @pl.when(jnp.logical_not(prime) & (odd == 0))
    def _():
        own_up(2)

    @pl.when(prime | (odd == 1))
    def _():
        own_down(2)

    done = jnp.maximum(me - 2, 0)

    @pl.when(jnp.logical_not(prime))
    def _():
        resid_passes(lambda copy: copy.start(), True)
        for number in range(2):
            attn_passes(number, lambda copy: copy.start(), True)


    def drain(first, last):
        lax.fori_loop(first, last, lambda number, carry: (event(number), carry)[1], 0)
        return jnp.maximum(first, last)


    @pl.when(prime)
    def _():
        resid_keep.wait()

    projection_keep.wait()
    for tp in range(owners):

        @pl.when(jnp.where(prime, tp != col, lax.div(tp, 2) != x))
        def _():
            send(resid, resid_at(tp), r_send.at[0, 0], r_recv.at[tp], me, twin).wait_recv()
            for number in range(2):
                send(outs[number], arrived[number].at[tp], a_send.at[number, 0, 0],
                     a_recv.at[number, tp], me, twin).wait_recv()

        size_a, size_b = outs[0].shape[1], outs[1].shape[1]
        large_from = owners * size_b
        joined[:, tp * size_b : (tp + 1) * size_b] = arrived[1][tp]
        joined[:, large_from + tp * size_a : large_from + (tp + 1) * size_a] = arrived[0][tp]

    features = projection.shape[0]

    def project(part, squares):
        number = done + part

        @pl.when(number < 2 * blocks - 2)
        def _():
            event(number)

        at = pl.ds(pl.multiple_of(part * TILE, TILE), TILE)
        mixed = jnp.dot(joined[:, :features], projection[:, at], preferred_element_type=jnp.float32)
        rounded = (resid_all[:, at].astype(jnp.float32) + mixed).astype(jnp.bfloat16)
        middle[:, at] = rounded
        wide = rounded.astype(jnp.float32)
        return squares + jnp.sum(wide * wide, axis=1, keepdims=True)

    squares = lax.fori_loop(0, width // TILE, project, jnp.zeros((rows, 1), jnp.float32))
    done = jnp.maximum(done, jnp.minimum(done + width // TILE, 2 * blocks - 2))
    scaling = lax.rsqrt(squares * (1.0 / width) + EPSILON)

    def normalise(part, carry):
        at = pl.ds(pl.multiple_of(part * TILE, TILE), TILE)
        scaled = middle[:, at].astype(jnp.float32) * scaling
        mixer[:, at] = (scaled * gain[:, at].astype(jnp.float32)).astype(jnp.bfloat16)
        return carry

    lax.fori_loop(0, width // TILE, normalise, 0)

    def share_middle():
        at = pl.ds(pl.multiple_of(twin * mine, mine), mine)
        return send(middle.at[at], kept, m_send, m_recv, me, twin)

    @pl.when(prime)
    def _():
        share_middle().start()
        kept[...] = middle[pl.ds(pl.multiple_of(col * mine, mine), mine), :]

    def ready(which, first):
        last = drain(first, (which + 1) * blocks)

        @pl.when(prime)
        def _():
            pltpu.make_async_copy(weights[which], slab(which, me), own_sem.at[which]).wait()

        @pl.when(jnp.logical_not(prime))
        def _():
            lax.fori_loop(0, count, lambda src, carry: (weight_wait(which, src), carry)[1], 0)

        return last

    spans = hidden // TILE

    def over_hidden(body):
        def step(part, carry):
            body(pl.ds(pl.multiple_of(part * TILE, TILE), TILE))
            return carry

        lax.fori_loop(0, spans, step, 0)
        if hidden % TILE:
            body(pl.ds(spans * TILE, hidden % TILE))

    done = ready(0, done)

    def gate_part(at):
        gated[:, at] = jnp.dot(mixer[...], whole[0, :, at], preferred_element_type=jnp.float32)

    over_hidden(gate_part)
    done = ready(1, done)

    def up_part(at):
        value = jnp.dot(mixer[...], whole[1, :, at], preferred_element_type=jnp.float32)
        opened = gated[:, at]
        joined[:, at] = (opened / (1.0 + jnp.exp(-opened)) * value).astype(jnp.bfloat16)

    over_hidden(up_part)
    done = drain(done, 2 * blocks)

    span = 2 * mine

    def columns_of(turn):
        src = jnp.where(turn == 0, me, place_of(jnp.maximum(turn - 1, 0))[3])
        return src, pl.ds(pl.multiple_of(src * depth, depth), depth)

    def row_span(pair):
        return pl.ds(pl.multiple_of(pair * span, span), span)

    def part_swap(turn, ahead):
        to = lax.rem(x + ahead, pairs)
        at = columns_of(turn)[1]
        return send(resid_all.at[row_span(to), at], halves.at[ahead - 1, :, at],
                    s_send.at[turn, ahead - 1], s_recv.at[turn, ahead - 1], me, to * 2 + core)

    def part_send(turn, side):
        at = columns_of(turn)[1]
        rows_at = pl.ds(pl.multiple_of((x * 2 + side) * mine, mine), mine)
        return send(resid_all.at[rows_at, at], parts.at[odd, :, at],
                    p_send.at[side], p_recv.at[odd], token, x * 2 + side)

    def combine(turn):
        at = columns_of(turn)[1]
        total = resid_all[row_span(x), at].astype(jnp.float32)
        for ahead in range(1, pairs):
            part_swap(turn, ahead).wait_recv()
            total = total + halves[ahead - 1, :, at].astype(jnp.float32)
        resid_all[row_span(x), at] = total.astype(jnp.bfloat16)
        for side in range(2):
            local = prime & (side == core)

            @pl.when(jnp.logical_not(local))
            def _():
                part_send(turn, side).start()

            @pl.when(local)
            def _():
                parts[odd, :, at] = total[side * mine : (side + 1) * mine].astype(jnp.bfloat16)

    def lower(turn, carry):
        src, at = columns_of(turn)

        @pl.when(prime & (turn == 0))
        def _():
            pltpu.make_async_copy(weights[2], slab(2, me), own_sem.at[2]).wait()

        @pl.when(prime & (2 * blocks + turn > done))
        def _():
            event(2 * blocks + turn - 1)

        @pl.when(jnp.logical_not(prime))
        def _():
            weight_wait(2, src)

        partial = lax.dot_general(
            joined[:, :hidden], whole[2, at, :], (((1,), (1,)), ((), ())),
            preferred_element_type=jnp.float32,
        ).astype(jnp.bfloat16)
        resid_all[:, at] = partial
        for ahead in range(1, pairs):
            part_swap(turn, ahead).start()

        pl.when(turn > 0)(lambda: combine(turn - 1))
        return carry

    @pl.when(jnp.logical_not(prime))
    def _():
        resid_passes(lambda copy: copy.wait_send(), False)

    lax.fori_loop(0, count, lower, 0)
    combine(count - 1)

    resid_sends(lambda copy: copy.wait_send())
    for number in range(2):
        attn_sends(number, lambda copy: copy.wait_send())

    @pl.when(jnp.logical_not(prime))
    def _():
        for number in range(2):
            attn_passes(number, lambda copy: copy.wait_send(), False)

    def swap_close(turn, carry):
        for ahead in range(1, pairs):
            part_swap(turn, ahead).wait_send()
        return carry

    lax.fori_loop(0, count, swap_close, 0)
    for side in range(2):
        rows_at = pl.ds(pl.multiple_of((x * 2 + side) * mine, mine), mine)
        copy = send(resid_all.at[rows_at], parts.at[side], p_send.at[side], p_recv.at[side], me, twin)

        @pl.when(jnp.logical_not(prime) | (side != core))
        def _():
            copy.wait_send()

        @pl.when(jnp.logical_not(prime) | (side != odd))
        def _():
            copy.wait_recv()

    @pl.when(prime)
    def _():
        share_middle().wait_send()

    @pl.when(jnp.logical_not(prime))
    def _():
        share_middle().wait_recv()

    total = kept[...].astype(jnp.float32)
    for tp in range(2):
        total = total + parts[tp].astype(jnp.float32)
    result[...] = total.astype(jnp.bfloat16)

    latent_own(lambda copy: copy.wait_send())

    def latent_close(step, carry):
        @pl.when(step <= z)
        def _():
            latent_row(step, lambda copy: copy.wait_send())

        src, straight = latent_source(step)

        @pl.when(jnp.logical_not(straight) & jnp.logical_not(prime))
        def _():
            latent_twin(src).wait_send()

        return carry

    lax.fori_loop(1, me + 1, latent_close, 0)

    def weight_close(which, carry):
        @pl.when(z + stride < tall)
        def _():
            weight_z(slab(which, me), which, me, w_z.at[which, 0], z + stride).wait_send()

        @pl.when(z - stride >= 0)
        def _():
            weight_z(slab(which, me), which, me, w_z.at[which, 1], z - stride).wait_send()

        @pl.when(prime)
        def _():
            for place in range(tall):
                zs = listed(place)

                @pl.when(((zs < z) & (z + 2 < tall)) | ((zs > z) & (z - 2 >= 0)))
                def _():
                    weight_z(slab(which, me), which, me, w_zr.at[which, place], z).wait_send()

                for ahead in range(1, deep):
                    weight_y(slab(which, me), which, me, w_y.at[which, place, ahead - 1], ahead).wait_send()

            for index in range(count):
                weight_twin(slab(which, me), which, me, w_d.at[which, index]).wait_send()

        return carry

    lax.fori_loop(0, 3, weight_close, 0)


def on_device(
    count,
    owners,
    resid,
    query_small,
    query_large,
    kv_latent,
    rope_key,
    kv_gain,
    up_key_small,
    up_value_small,
    up_key_large,
    up_value_large,
    out_weight,
    mix_gain,
    gate_weight,
    up_weight,
    down_weight,
):
    rows, latent_size = kv_latent.shape
    mine, width = resid.shape
    offset = lax.axis_index("sp") * rows
    positions = offset + jnp.arange(rows, dtype=jnp.int32)
    angle_cos, angle_sin = angles(positions, ROTARY)
    half = rows // 2
    pieces = latent_size // ROTARY
    thick = half // pieces
    spun = rotate(rope_key, angle_cos, angle_sin).reshape(2, pieces, thick, ROTARY)
    shared = jnp.concatenate(
        [
            norm_rows(kv_latent, kv_gain).reshape(2, half, latent_size),
            jnp.transpose(spun, (0, 2, 1, 3)).reshape(2, thick, latent_size),
        ],
        axis=1,
    )

    passes = []
    queries, keys, values = [], [], []
    key_at = value_at = 0
    for query, up_key, up_value, nope, size in (
        (query_large, up_key_large, up_value_large, NOPE_LARGE, VALUE_LARGE),
        (query_small, up_key_small, up_value_small, NOPE_SMALL, VALUE_SMALL),
    ):
        heads = up_key.shape[1] // nope
        wide = nope + ROTARY
        padded = nope // LANES * LANES + LANES
        gap = padded - LANES + SPIN - nope
        shaped = query.reshape(rows, heads, wide)
        turned = rotate(shaped[..., nope:], angle_cos[:, None, :], angle_sin[:, None, :])
        empty = jnp.zeros((rows, heads, gap), jnp.bfloat16)
        full = jnp.concatenate([shaped[..., :nope], empty, turned], axis=-1)
        full = jnp.pad(full, ((0, 0), (0, 0), (0, padded - wide - gap)))
        queries.append(jnp.transpose(full, (1, 2, 0)))
        held = -(-nope // LANES) * LANES
        group = []
        for head in range(heads):
            keys.append(jnp.pad(up_key[:, head * nope : (head + 1) * nope], ((0, 0), (0, held - nope))))
            group.append((head, nope, held, key_at, size, value_at, head * (size + PAD)))
            key_at += held
            value_at += size
        passes.append(tuple(group))
        values.append(jnp.transpose(up_value))
    expand_key = jnp.concatenate(keys, axis=1)
    expand_value = jnp.concatenate(values, axis=0)
    depth, hidden = gate_weight.shape
    features = out_weight.shape[0]
    sizes = [len(group) * group[0][4] for group in passes]
    most = max(len(group) for group in passes)
    tallest = max(len(group) * (group[0][4] + PAD) for group in passes)
    deep = 1 << ((count.bit_length() - 1) // 2)
    tall = count // deep
    pairs = owners // 2
    vmem = pl.BlockSpec(memory_space=pltpu.VMEM)
    hbm = pl.BlockSpec(memory_space=pl.ANY)
    bf16, f32 = jnp.bfloat16, jnp.float32
    dma = pltpu.SemaphoreType.DMA
    return pl.pallas_call(
        functools.partial(layer, count, owners, tuple(passes)),
        out_shape=jax.ShapeDtypeStruct((mine, width), bf16),
        in_specs=[hbm, vmem, vmem, hbm, vmem, hbm, hbm, hbm, hbm, vmem, vmem],
        out_specs=vmem,
        scratch_shapes=[
            pltpu.VMEM((count,) + shared.shape, bf16),
            pltpu.VMEM((count * rows, LANES), bf16),
            pltpu.VMEM((3, count * depth, hidden), bf16),
            pltpu.VMEM((owners, rows, sizes[0]), bf16),
            pltpu.VMEM((owners, rows, sizes[1]), bf16),
            pltpu.VMEM((rows, sizes[0]), bf16),
            pltpu.VMEM((rows, sizes[1]), bf16),
            pltpu.VMEM((rows, max(features, hidden)), bf16),
            pltpu.VMEM((features, width), bf16),
            pltpu.VMEM((owners * mine, width), bf16),
            pltpu.VMEM((rows, width), bf16),
            pltpu.VMEM((rows, width), bf16),
            pltpu.VMEM((rows, hidden), f32),
            pltpu.VMEM((2, mine, width), bf16),
            pltpu.VMEM((mine, width), bf16),
            pltpu.VMEM((most, 1, rows), f32),
            pltpu.VMEM((tallest, rows), f32),
            dma((count,)),
            dma((tall,)),
            dma((tall, deep)),
            dma((count,)),
            dma((3, count)),
            dma((3, 2)),
            dma((3, tall)),
            dma((3, tall, deep)),
            dma((3, count)),
            dma((6,)),
            dma((2, pairs)),
            dma((owners,)),
            dma((2, pairs)),
            dma((2, 2, pairs)),
            dma((2, owners)),
            dma((2, 2, pairs)),
            dma((count, pairs)),
            dma((count, pairs)),
            dma,
            dma,
            dma((2,)),
            dma((2,)),
            pltpu.VMEM((pairs - 1, 2 * mine, width), bf16),
        ],
        compiler_params=pltpu.CompilerParams(
            collective_id=0, has_side_effects=True, vmem_limit_bytes=67043328
        ),
        cost_estimate=pl.CostEstimate(
            flops=10**11, bytes_accessed=3 * 10**7, transcendentals=2 * 10**7
        ),
    )(
        shared,
        expand_key,
        expand_value,
        resid,
        mix_gain.reshape(1, width),
        out_weight,
        gate_weight,
        up_weight,
        down_weight,
        queries[0],
        queries[1],
    )


def solution(mesh):
    placed = (
        P(("sp", "tp"), None),
        P("sp", "tp"),
        P("sp", "tp"),
        P("sp", None),
        P("sp", None),
        P(),
        P(None, "tp"),
        P(None, "tp"),
        P(None, "tp"),
        P(None, "tp"),
        P(),
        P(),
        P("sp", "tp"),
        P("sp", "tp"),
        P("sp", "tp"),
    )
    return jax.shard_map(
        functools.partial(on_device, mesh.shape["sp"], mesh.shape["tp"]), mesh=mesh, in_specs=placed, out_specs=P(("sp", "tp"), None), check_vma=False
    )
```

```python
import functools
import math

import jax
import jax.numpy as jnp
from jax import lax
from jax.experimental import pallas as pl
from jax.experimental.pallas import tpu as pltpu
from jax.sharding import PartitionSpec as P

HEADS_SMALL = 8
NOPE_SMALL = 64
NOPE_LARGE = 128
VALUE_SMALL = 64
VALUE_LARGE = 128
ROTARY = 32


THETA = 10000.0
EPSILON = 1e-06
FLOOR = -1e30


LOG2E = math.log2(math.e)
TILE = 256
PAD = 16
LANES = 128
SPIN = NOPE_SMALL


def layer(count, owners, passes, *refs):
    (resid, gain, out_weight) = refs[:3]
    weights = refs[3:6]
    (fresh, spinning, fresh_gain, turns) = refs[6:10]
    asked, raised, valued = refs[10:12], refs[12:14], refs[14:16]
    result = refs[16]
    queries, lifted = refs[-6:-4], refs[-3:-1]
    keyed = tuple(raised[n] if passes[n][0][1] % LANES == 0 else refs[-4] for n in range(2))
    refs = refs[:6] + refs[11:]
    (kv, turned, whole, arrived_a, arrived_b, outs_a, outs_b, joined, projection, resid_all, middle) = refs[12:23]
    (mixer, gated, parts, kept, maxima, sums) = refs[23:29]
    (kv_recv, kv_up, kv_y, kv_d, w_recv, w_z, w_zr, w_y, w_d, own_sem) = refs[29:39]
    (r_send, r_recv, r_pass, a_send, a_recv, a_pass, s_send, s_recv) = refs[39:47]
    (m_send, m_recv, p_send, p_recv, halves) = refs[47:52]
    arrived, outs = (arrived_a, arrived_b), (outs_a, outs_b)

    deep = 1 << ((count.bit_length() - 1) // 2)
    tall = count // deep
    pairs = owners // 2
    blocks = count - 1
    me = lax.axis_index("sp")
    col = lax.axis_index("tp")
    z, y = lax.div(me, deep), lax.rem(me, deep)
    x, core = lax.div(col, 2), lax.rem(col, 2)
    odd = lax.rem(z, 2)
    prime = core == odd
    other = z + 1 - 2 * odd
    token = (z - odd + core) * deep + y
    group = x * 2 + odd
    twin = x * 2 + 1 - core
    rows = fresh.shape[0]
    depth, hidden = weights[0].shape
    mine = resid.shape[0]
    width = resid.shape[1]
    half = rows // 2

    def send(source, target, out_sem, in_sem, sp, tp):
        return pltpu.make_async_remote_copy(
            src_ref=source,
            dst_ref=target,
            send_sem=out_sem,
            recv_sem=in_sem,
            device_id={"sp": sp, "tp": tp},
            device_id_type=pl.DeviceIdType.MESH,
        )

    barrier = pltpu.get_barrier_semaphore()

    def greet(sp, tp):
        pl.semaphore_signal(
            barrier, inc=1, device_id={"sp": sp, "tp": tp}, device_id_type=pl.DeviceIdType.MESH
        )

    for ahead in range(1, tall):
        greet(lax.rem(z + ahead, tall) * deep + y, col)
    for ahead in range(1, deep):
        greet(z * deep + lax.rem(y + ahead, deep), col)
    for ahead in range(1, owners):
        greet(me, lax.rem(col + ahead, owners))
        greet(other * deep + y, lax.rem(col + ahead, owners))
    greet(lax.rem(z - 1 + 2 * odd + tall, tall) * deep + y, twin)
    wide = fresh[...].astype(jnp.float32)
    scaled = wide * lax.rsqrt(jnp.mean(wide * wide, axis=-1, keepdims=True) + EPSILON)
    normed = (scaled * fresh_gain[...].astype(jnp.float32)[None, :]).astype(jnp.bfloat16)
    for part in range(2):
        kv[me, part, :half] = normed[part * half : (part + 1) * half]

    def flipped(values):
        short = -values.shape[1] % LANES
        wide = values.astype(jnp.float32)
        if short:
            wide = jnp.concatenate([wide, jnp.zeros((values.shape[0], short), jnp.float32)], axis=1)
        return wide.T

    def spin(first, second):
        angle_cos, angle_sin = turns[0], turns[1]
        return jnp.concatenate(
            [first * angle_cos - second * angle_sin, second * angle_cos + first * angle_sin], axis=0
        )

    small = ROTARY // 2
    upright = spinning[...].astype(jnp.float32)
    rotated = spin(upright[:small], upright[small:])
    rotated = jnp.concatenate(
        [
            jnp.zeros((SPIN, rows), jnp.float32),
            rotated,
            jnp.zeros((LANES - SPIN - ROTARY, rows), jnp.float32),
        ],
        axis=0,
    ).T.astype(jnp.bfloat16)
    turned[pl.ds(pl.multiple_of(me * rows, rows), rows), :] = rotated
    thick = kv.shape[2] - half
    for part in range(2):
        for piece in range(half // thick):
            at = part * half + piece * thick
            kv[me, part, half:, piece * ROTARY : (piece + 1) * ROTARY] = (
                rotated[at : at + thick, SPIN : SPIN + ROTARY]
            )

    pl.semaphore_wait(barrier, tall - 1 + deep - 1 + 2 * (owners - 1) + 1)

    def latent_up(source, src, away):
        lead = x * 2 + 1 - odd
        return send(source, kv.at[src], kv_up.at[away], kv_recv.at[src], me + deep, lead)

    def latent_over(source, src, away, ahead):
        to = z * deep + lax.rem(y + ahead, deep)
        return send(source, kv.at[src], kv_y.at[away, ahead - 1], kv_recv.at[src], to, col)

    def latent_twin(src):
        return send(kv.at[src], kv.at[src], kv_d.at[src], kv_recv.at[src], me, twin)

    def latent_own(act):
        @pl.when(prime & (z + 1 < tall))
        def _():
            act(latent_up(kv.at[me], me, 0))

        for ahead in range(1, deep):

            @pl.when(jnp.logical_not(prime) & (y + ahead < deep))
            def _():
                act(latent_over(kv.at[me], me, 0, ahead))

    def latent_row(away, act):
        src = me - away * deep

        @pl.when(prime)
        def _():
            @pl.when(z + 1 < tall)
            def _():
                act(latent_up(kv.at[src], src, away))

            act(latent_twin(src))

        @pl.when(jnp.logical_not(prime))
        def _():
            for ahead in range(1, deep):
                act(latent_over(kv.at[src], src, away, ahead))

    def latent_source(step):
        rest = jnp.maximum(step - y - 1, 0)
        spot = lax.rem(rest, deep)
        near = step <= y
        level = jnp.where(near, 0, 1 + lax.div(rest, deep))
        over = jnp.where(near, y - step, lax.rem(y + spot, deep))
        return (z - level) * deep + over, jnp.logical_not(near) & (spot == 0)

    latent_own(lambda copy: copy.start())

    def latent_step(step):
        @pl.when(step <= z)
        def _():
            latent_twin(me - step * deep).wait_recv()
            latent_row(step, lambda copy: copy.start())

        src, straight = latent_source(step)

        @pl.when(jnp.logical_not(straight))
        def _():
            latent_twin(src).wait_recv()

            @pl.when(jnp.logical_not(prime))
            def _():
                latent_twin(src).start()

    def listed(place):
        rising = jnp.where(place - 1 < z, place - 1, place)
        falling = jnp.where(tall - place > z, tall - place, tall - 1 - place)
        return jnp.where(place == 0, z, jnp.where(z < tall // 2, rising, falling))

    def slab(which, src):
        return whole.at[which, pl.ds(pl.multiple_of(src * depth, depth), depth)]

    def weight_z(source, which, src, sem, to):
        return send(source, slab(which, src), sem, w_recv.at[which, src], to * deep + y, col)

    def weight_y(source, which, src, sem, ahead):
        to = z * deep + lax.rem(y + ahead, deep)
        return send(source, slab(which, src), sem, w_recv.at[which, src], to, col)

    def weight_twin(source, which, src, sem):
        return send(source, slab(which, src), sem, w_recv.at[which, src], me, twin)

    def weight_wait(which, src):
        weight_twin(slab(which, src), which, src, w_d.at[which, 0]).wait_recv()

    stride = jnp.where(prime, 2, 1)

    def own_up(which):
        @pl.when(z + stride < tall)
        def _():
            weight_z(weights[which], which, me, w_z.at[which, 0], z + stride).start()

    def own_down(which):
        @pl.when(z - stride >= 0)
        def _():
            weight_z(weights[which], which, me, w_z.at[which, 1], z - stride).start()

    def own_over(which):
        source = weights[which]

        @pl.when(prime)
        def _():
            for ahead in range(1, deep):
                weight_y(source, which, me, w_y.at[which, 0, ahead - 1], ahead).start()
            weight_twin(source, which, me, w_d.at[which, 0]).start()
            pltpu.make_async_copy(source, slab(which, me), own_sem.at[which]).start()

    def place_of(index):
        turn, spot = lax.div(index, deep), lax.rem(index, deep)
        final = turn == tall - 1
        straight = (spot == 0) & (turn < tall - 1)
        place = jnp.where(straight, turn + 1, turn)
        over = jnp.where(straight, 0, jnp.where(final, spot + 1, spot))
        zs = listed(place)
        return straight, place, zs, zs * deep + lax.rem(y + over, deep)

    def relay(which, index):
        straight, place, zs, src = place_of(index)
        weight_wait(which, src)
        block = slab(which, src)

        @pl.when(straight)
        def _():
            @pl.when((zs < z) & (z + 2 < tall))
            def _():
                weight_z(block, which, src, w_zr.at[which, place], z + 2).start()

            @pl.when((zs > z) & (z - 2 >= 0))
            def _():
                weight_z(block, which, src, w_zr.at[which, place], z - 2).start()

            for ahead in range(1, deep):
                weight_y(block, which, src, w_y.at[which, place, ahead - 1], ahead).start()

        weight_twin(block, which, src, w_d.at[which, index + 1]).start()

    def event(number):
        @pl.when(prime & (number == 3))
        def _():
            own_up(1)

        @pl.when(prime & (number == 4))
        def _():
            own_over(2)

        @pl.when(prime & (number == blocks + 3))
        def _():
            own_up(2)
            own_down(2)

        @pl.when(prime & (number < 3 * blocks))
        def _():
            relay(lax.div(number, blocks), lax.rem(number, blocks))

    def targets():
        for far in range(2):
            for ahead in range(pairs):
                block = me if far == 0 else other * deep + y
                yield far, ahead, block, lax.rem(x + ahead, pairs) * 2 + odd

    def share(far, ahead, copy):
        if far == 0 and ahead == 0:

            @pl.when(jnp.logical_not(prime))
            def _():
                copy()
        else:
            copy()

    def resid_at(tp):
        return resid_all.at[pl.ds(pl.multiple_of(tp * mine, mine), mine)]

    def resid_sends(act, which):
        for far, ahead, sp, tp in targets():
            if far in which and (far == 0 or ahead == 0):
                share(far, ahead, lambda: act(
                    send(resid, resid_at(col), r_send.at[far, ahead], r_recv.at[col], sp, tp)))

    def resid_passes(act, wait):
        for side in range(2):
            source = x * 2 + side
            block = resid_at(source)
            if wait:
                send(block, block, r_pass.at[side, 0], r_recv.at[source], me, twin).wait_recv()
            for ahead in range(1, pairs):
                act(send(block, block, r_pass.at[side, ahead], r_recv.at[source],
                         me, lax.rem(x + ahead, pairs) * 2 + core))

    def attn_sends(number, act):
        for far, ahead, sp, tp in targets():
            if far == 0 or ahead == 0:
                share(far, ahead, lambda: act(
                    send(outs[number], arrived[number].at[col], a_send.at[number, far, ahead],
                         a_recv.at[number, col], sp, tp)))

    def attn_passes(number, act, wait):
        for side in range(2):
            source = x * 2 + side
            block = arrived[number].at[source]
            if wait:
                send(block, block, a_pass.at[number, side, 0], a_recv.at[number, source], me, twin).wait_recv()
            for ahead in range(1, pairs):
                act(send(block, block, a_pass.at[number, side, ahead], a_recv.at[number, source],
                         me, lax.rem(x + ahead, pairs) * 2 + core))

    def early_up():
        own_up(0)

        @pl.when(odd == 0)
        def _():
            resid_sends(lambda copy: copy.start(), (1,))

    resid_sends(lambda copy: copy.start(), (0,))
    own_down(0)
    own_over(0)
    pl.when(jnp.logical_not(prime) & (z > 0))(early_up)

    @pl.when(odd == 1)
    def _():
        resid_sends(lambda copy: copy.start(), (1,))

    @pl.when(jnp.logical_not(prime))
    def _():
        own_down(1)

    def first_up():
        pl.when((prime & (odd == 1)) | (z == 0))(early_up)

        @pl.when(jnp.logical_not(prime) & (odd == 1))
        def _():
            own_up(1)

    resid_keep = pltpu.make_async_copy(
        resid, resid_all.at[pl.ds(pl.multiple_of(col * mine, mine), mine)], own_sem.at[4]
    )

    @pl.when(prime)
    def _():
        resid_keep.start()

    projection_keep = pltpu.make_async_copy(out_weight, projection, own_sem.at[5])
    projection_keep.start()

    for number, group in enumerate(passes):
        upright = asked[number]
        tall_values = flipped(valued[number][...])
        for inner, nope, held, size, sum_at in group:
            base = inner * (nope + ROTARY)
            whole_query = queries[number].shape[1]
            gap = whole_query - LANES + SPIN
            queries[number][inner, :nope, :] = upright[base : base + nope, :]
            if gap > nope:
                queries[number][inner, nope:gap, :] = jnp.zeros((gap - nope, rows), jnp.bfloat16)
            queries[number][inner, gap : gap + ROTARY, :] = spin(
                upright[base + nope : base + nope + small, :].astype(jnp.float32),
                upright[base + nope + small : base + nope + ROTARY, :].astype(jnp.float32),
            ).astype(jnp.bfloat16)
            queries[number][inner, gap + ROTARY :, :] = jnp.zeros(
                (whole_query - gap - ROTARY, rows), jnp.bfloat16
            )
            lifted[number][inner * size : (inner + 1) * size, :] = (
                tall_values[inner * size : (inner + 1) * size].astype(jnp.bfloat16)
            )
            if nope % LANES:
                piece = raised[number][:, inner * nope : (inner + 1) * nope]
                blank = jnp.zeros((piece.shape[0], held - nope), jnp.bfloat16)
                keyed[number][:, inner * held : (inner + 1) * held] = jnp.concatenate([piece, blank], axis=1)


    def unpack(index):
        for part in range(2):
            packed = kv[index, part, half:]
            thick = packed.shape[0]
            for piece in range(half // thick):
                slim = packed[:, piece * ROTARY : (piece + 1) * ROTARY]
                before = jnp.zeros((thick, SPIN), jnp.bfloat16)
                after = jnp.zeros((thick, LANES - SPIN - ROTARY), jnp.bfloat16)
                turned[pl.ds(pl.multiple_of(index * rows + part * half + piece * thick, thick), thick), :] = (
                    jnp.concatenate([before, slim, after], axis=1)
                )

    def tiles(number, index, diagonal):
        latent = jnp.concatenate([kv[index, 0, :half], kv[index, 1, :half]], axis=0)
        spun = turned[pl.ds(pl.multiple_of(index * rows, rows), rows), :]
        for head, (inner, nope, held, size, sum_at) in enumerate(passes[number]):
            key = jnp.dot(
                latent, keyed[number][:, inner * held : (inner + 1) * held], preferred_element_type=jnp.float32
            ).astype(jnp.bfloat16)
            key = jnp.concatenate([key, spun], axis=1) if nope % LANES == 0 else key + spun
            value = lax.dot_general(
                lifted[number][inner * size : (inner + 1) * size, :],
                latent,
                (((1,), (1,)), ((), ())),
                preferred_element_type=jnp.float32,
            ).astype(jnp.bfloat16)
            value = jnp.concatenate([value, jnp.ones((PAD, rows), jnp.bfloat16)], axis=0)
            scale = LOG2E / math.sqrt(nope + ROTARY)
            for tile in range(rows // TILE):
                columns = slice(tile * TILE, (tile + 1) * TILE)
                length = (tile + 1) * TILE if diagonal else rows
                scores = jnp.dot(
                    key[:length], queries[number][inner, :, columns], preferred_element_type=jnp.float32
                )
                place = slice(sum_at, sum_at + size + PAD)
                if diagonal:
                    key_pos = lax.broadcasted_iota(jnp.int32, scores.shape, 0)
                    query_pos = lax.broadcasted_iota(jnp.int32, scores.shape, 1) + tile * TILE
                    scores = jnp.where(key_pos <= query_pos, scores, FLOOR)
                    new = jnp.max(scores, axis=0, keepdims=True)
                    weight = jnp.exp2((scores - new) * scale).astype(jnp.bfloat16)
                    maxima[head, :, columns] = new
                    sums[place, columns] = jnp.dot(
                        value[:, :length], weight, preferred_element_type=jnp.float32
                    )
                else:
                    old = maxima[head, :, columns]
                    new = jnp.maximum(old, jnp.max(scores, axis=0, keepdims=True))
                    weight = jnp.exp2((scores - new) * scale).astype(jnp.bfloat16)
                    factor = jnp.exp2((old - new) * scale)
                    maxima[head, :, columns] = new
                    sums[place, columns] = sums[place, columns] * factor + jnp.dot(
                        value, weight, preferred_element_type=jnp.float32
                    )

    def finish(number):
        for inner, nope, held, size, sum_at in passes[number]:
            for tile in range(rows // TILE):
                columns = slice(tile * TILE, (tile + 1) * TILE)
                total = sums[sum_at : sum_at + size, columns] / sums[sum_at + size : sum_at + size + 1, columns]
                outs[number][columns, inner * size : (inner + 1) * size] = total.T.astype(jnp.bfloat16)
        attn_sends(number, lambda copy: copy.start())

        @pl.when(prime)
        def _():
            arrived[number][col] = outs[number][...]

    tiles(0, me, True)

    def first_step(step, carry):
        latent_step(step)

        pl.when(prime & (odd == 0) & (step == z))(early_up)

        @pl.when(step == 4)
        def _():
            event(0)

        @pl.when(prime & (step == jnp.minimum(me, 4)))
        def _():
            own_down(1)

        src, straight = latent_source(step)
        unpack(src)
        tiles(0, src, False)
        return carry

    lax.fori_loop(1, me + 1, first_step, 0)
    finish(0)

    first_up()
    own_over(1)
    tiles(1, me, True)

    started = jnp.where(me < 4, 1, 0)

    def second_step(step, carry):
        @pl.when(step < 6)
        def _():
            event(step - started)

        @pl.when(jnp.logical_not(prime) & (step == 5))
        def _():
            resid_passes(lambda copy: copy.start(), True)

        @pl.when(jnp.logical_not(prime) & (step == 6))
        def _():
            attn_passes(0, lambda copy: copy.start(), True)

        tiles(1, me - step, False)
        return carry

    lax.fori_loop(1, me + 1, second_step, 0)
    finish(1)

    @pl.when(jnp.logical_not(prime))
    def _():
        pl.when(odd == 0)(lambda: own_up(1))

    done = jnp.minimum(me, 5) + 1 - started

    def drain(first, last):
        lax.fori_loop(first, last, lambda number, carry: (event(number), carry)[1], 0)
        return jnp.maximum(first, last)

    done = drain(done, jnp.where(z == tall - 1, done, blocks))

    @pl.when(jnp.logical_not(prime))
    def _():
        @pl.when(me < 5)
        def _():
            resid_passes(lambda copy: copy.start(), True)

        @pl.when(me < 6)
        def _():
            attn_passes(0, lambda copy: copy.start(), True)

        attn_passes(1, lambda copy: copy.start(), True)


    @pl.when(jnp.logical_not(prime))
    def _():
        own_up(2)
        own_down(2)


    @pl.when(prime)
    def _():
        resid_keep.wait()

    projection_keep.wait()
    for tp in range(owners):

        @pl.when(jnp.where(prime, tp != col, lax.div(tp, 2) != x))
        def _():
            send(resid, resid_at(tp), r_send.at[0, 0], r_recv.at[tp], me, twin).wait_recv()
            for number in range(2):
                send(outs[number], arrived[number].at[tp], a_send.at[number, 0, 0],
                     a_recv.at[number, tp], me, twin).wait_recv()

        size_a, size_b = outs[0].shape[1], outs[1].shape[1]
        large_from = owners * size_b
        joined[:, tp * size_b : (tp + 1) * size_b] = arrived[1][tp]
        joined[:, large_from + tp * size_a : large_from + (tp + 1) * size_a] = arrived[0][tp]

    features = projection.shape[0]

    def project(part, squares):
        number = done + part

        @pl.when(number < 2 * blocks - 2)
        def _():
            event(number)

        at = pl.ds(pl.multiple_of(part * TILE, TILE), TILE)
        mixed = jnp.dot(joined[:, :features], projection[:, at], preferred_element_type=jnp.float32)
        rounded = (resid_all[:, at].astype(jnp.float32) + mixed).astype(jnp.bfloat16)
        middle[:, at] = rounded
        wide = rounded.astype(jnp.float32)
        return squares + jnp.sum(wide * wide, axis=1, keepdims=True)

    squares = lax.fori_loop(0, width // TILE, project, jnp.zeros((rows, 1), jnp.float32))
    done = jnp.maximum(done, jnp.minimum(done + width // TILE, 2 * blocks - 2))
    scaling = lax.rsqrt(squares * (1.0 / width) + EPSILON)

    def normalise(part, carry):
        at = pl.ds(pl.multiple_of(part * TILE, TILE), TILE)
        scaled = middle[:, at].astype(jnp.float32) * scaling
        mixer[:, at] = (scaled * gain[at].astype(jnp.float32)[None, :]).astype(jnp.bfloat16)
        return carry

    lax.fori_loop(0, width // TILE, normalise, 0)

    def share_middle():
        at = pl.ds(pl.multiple_of(twin * mine, mine), mine)
        return send(middle.at[at], kept, m_send, m_recv, me, twin)

    @pl.when(prime)
    def _():
        share_middle().start()
        kept[...] = middle[pl.ds(pl.multiple_of(col * mine, mine), mine), :]

    def ready(which, first):
        last = drain(first, (which + 1) * blocks)

        @pl.when(prime)
        def _():
            pltpu.make_async_copy(weights[which], slab(which, me), own_sem.at[which]).wait()

        @pl.when(jnp.logical_not(prime))
        def _():
            lax.fori_loop(0, count, lambda src, carry: (weight_wait(which, src), carry)[1], 0)

        return last

    spans = hidden // TILE

    def over_hidden(body):
        def step(part, carry):
            body(pl.ds(pl.multiple_of(part * TILE, TILE), TILE))
            return carry

        lax.fori_loop(0, spans, step, 0)
        if hidden % TILE:
            body(pl.ds(spans * TILE, hidden % TILE))

    done = ready(0, done)

    def gate_part(at):
        gated[:, at] = jnp.dot(mixer[...], whole[0, :, at], preferred_element_type=jnp.float32)

    over_hidden(gate_part)
    done = ready(1, done)

    def up_part(at):
        value = jnp.dot(mixer[...], whole[1, :, at], preferred_element_type=jnp.float32)
        opened = gated[:, at]
        joined[:, at] = (opened / (1.0 + jnp.exp(-opened)) * value).astype(jnp.bfloat16)

    over_hidden(up_part)
    done = drain(done, 2 * blocks)

    span = 2 * mine

    def columns_of(turn):
        src = jnp.where(turn == 0, me, place_of(jnp.maximum(turn - 1, 0))[3])
        return src, pl.ds(pl.multiple_of(src * depth, depth), depth)

    def row_span(pair):
        return pl.ds(pl.multiple_of(pair * span, span), span)

    def part_swap(turn, ahead):
        to = lax.rem(x + ahead, pairs)
        at = columns_of(turn)[1]
        return send(resid_all.at[row_span(to), at], halves.at[ahead - 1, :, at],
                    s_send.at[turn, ahead - 1], s_recv.at[turn, ahead - 1], me, to * 2 + core)

    def part_send(turn, side):
        at = columns_of(turn)[1]
        rows_at = pl.ds(pl.multiple_of((x * 2 + side) * mine, mine), mine)
        return send(resid_all.at[rows_at, at], parts.at[odd, :, at],
                    p_send.at[side], p_recv.at[odd], token, x * 2 + side)

    def combine(turn):
        at = columns_of(turn)[1]
        total = resid_all[row_span(x), at].astype(jnp.float32)
        for ahead in range(1, pairs):
            part_swap(turn, ahead).wait_recv()
            total = total + halves[ahead - 1, :, at].astype(jnp.float32)
        resid_all[row_span(x), at] = total.astype(jnp.bfloat16)
        for side in range(2):
            local = prime & (side == core)

            @pl.when(jnp.logical_not(local))
            def _():
                part_send(turn, side).start()

            @pl.when(local)
            def _():
                parts[odd, :, at] = total[side * mine : (side + 1) * mine].astype(jnp.bfloat16)

    def lower(turn, carry):
        src, at = columns_of(turn)

        @pl.when(prime & (turn == 0))
        def _():
            pltpu.make_async_copy(weights[2], slab(2, me), own_sem.at[2]).wait()

        @pl.when(prime & (2 * blocks + turn > done))
        def _():
            event(2 * blocks + turn - 1)

        @pl.when(jnp.logical_not(prime))
        def _():
            weight_wait(2, src)

        partial = lax.dot_general(
            joined[:, :hidden], whole[2, at, :], (((1,), (1,)), ((), ())),
            preferred_element_type=jnp.float32,
        ).astype(jnp.bfloat16)
        resid_all[:, at] = partial
        for ahead in range(1, pairs):
            part_swap(turn, ahead).start()

        pl.when(turn > 0)(lambda: combine(turn - 1))
        return carry

    @pl.when(jnp.logical_not(prime))
    def _():
        resid_passes(lambda copy: copy.wait_send(), False)

    lax.fori_loop(0, count, lower, 0)
    combine(count - 1)

    resid_sends(lambda copy: copy.wait_send(), (0, 1))
    for number in range(2):
        attn_sends(number, lambda copy: copy.wait_send())

    @pl.when(jnp.logical_not(prime))
    def _():
        for number in range(2):
            attn_passes(number, lambda copy: copy.wait_send(), False)

    def swap_close(turn, carry):
        for ahead in range(1, pairs):
            part_swap(turn, ahead).wait_send()
        return carry

    lax.fori_loop(0, count, swap_close, 0)
    for side in range(2):
        rows_at = pl.ds(pl.multiple_of((x * 2 + side) * mine, mine), mine)
        copy = send(resid_all.at[rows_at], parts.at[side], p_send.at[side], p_recv.at[side], me, twin)

        @pl.when(jnp.logical_not(prime) | (side != core))
        def _():
            copy.wait_send()

        @pl.when(jnp.logical_not(prime) | (side != odd))
        def _():
            copy.wait_recv()

    @pl.when(prime)
    def _():
        share_middle().wait_send()

    @pl.when(jnp.logical_not(prime))
    def _():
        share_middle().wait_recv()

    total = kept[...].astype(jnp.float32)
    for tp in range(2):
        total = total + parts[tp].astype(jnp.float32)
    result[...] = total.astype(jnp.bfloat16)

    latent_own(lambda copy: copy.wait_send())

    def latent_close(step, carry):
        @pl.when(step <= z)
        def _():
            latent_row(step, lambda copy: copy.wait_send())

        src, straight = latent_source(step)

        @pl.when(jnp.logical_not(straight) & jnp.logical_not(prime))
        def _():
            latent_twin(src).wait_send()

        return carry

    lax.fori_loop(1, me + 1, latent_close, 0)

    def weight_close(which, carry):
        @pl.when(z + stride < tall)
        def _():
            weight_z(slab(which, me), which, me, w_z.at[which, 0], z + stride).wait_send()

        @pl.when(z - stride >= 0)
        def _():
            weight_z(slab(which, me), which, me, w_z.at[which, 1], z - stride).wait_send()

        @pl.when(prime)
        def _():
            for place in range(tall):
                zs = listed(place)

                @pl.when(((zs < z) & (z + 2 < tall)) | ((zs > z) & (z - 2 >= 0)))
                def _():
                    weight_z(slab(which, me), which, me, w_zr.at[which, place], z).wait_send()

                for ahead in range(1, deep):
                    weight_y(slab(which, me), which, me, w_y.at[which, place, ahead - 1], ahead).wait_send()

            for index in range(count):
                weight_twin(slab(which, me), which, me, w_d.at[which, index]).wait_send()

        return carry

    lax.fori_loop(0, 3, weight_close, 0)


def on_device(
    count,
    owners,
    resid,
    query_small,
    query_large,
    kv_latent,
    rope_key,
    kv_gain,
    up_key_small,
    up_value_small,
    up_key_large,
    up_value_large,
    out_weight,
    mix_gain,
    gate_weight,
    up_weight,
    down_weight,
):
    rows, latent_size = kv_latent.shape
    mine, width = resid.shape
    positions = lax.axis_index("sp") * rows + jnp.arange(rows, dtype=jnp.int32)
    inverse = THETA ** (-jnp.arange(0, ROTARY, 2).astype(jnp.float32) / ROTARY)
    phase = inverse[:, None] * positions.astype(jnp.float32)[None, :]
    turns = jnp.stack([jnp.cos(phase), jnp.sin(phase)])
    half = rows // 2
    packed = half + half * ROTARY // latent_size

    passes = []
    for up_key, nope, size in (
        (up_key_large, NOPE_LARGE, VALUE_LARGE),
        (up_key_small, NOPE_SMALL, VALUE_SMALL),
    ):
        held = -(-nope // LANES) * LANES
        passes.append(tuple(
            (head, nope, held, size, head * (size + PAD)) for head in range(up_key.shape[1] // nope)
        ))
    depth, hidden = gate_weight.shape
    features = out_weight.shape[0]
    sizes = [len(group) * group[0][3] for group in passes]
    counts = [len(group) for group in passes]
    fulls = [group[0][1] // LANES * LANES + LANES for group in passes]
    most = max(len(group) for group in passes)
    tallest = max(len(group) * (group[0][3] + PAD) for group in passes)
    deep = 1 << ((count.bit_length() - 1) // 2)
    tall = count // deep
    pairs = owners // 2
    vmem = pl.BlockSpec(memory_space=pltpu.VMEM)
    hbm = pl.BlockSpec(memory_space=pl.ANY)
    bf16, f32 = jnp.bfloat16, jnp.float32
    dma = pltpu.SemaphoreType.DMA
    return pl.pallas_call(
        functools.partial(layer, count, owners, tuple(passes)),
        out_shape=jax.ShapeDtypeStruct((mine, width), bf16),
        in_specs=[hbm, vmem, hbm] + [hbm] * 3 + [vmem] * 10,
        out_specs=vmem,
        scratch_shapes=[
            pltpu.VMEM((count, 2, packed, latent_size), bf16),
            pltpu.VMEM((count * rows, LANES), bf16),
            pltpu.VMEM((3, count * depth, hidden), bf16),
            pltpu.VMEM((owners, rows, sizes[0]), bf16),
            pltpu.VMEM((owners, rows, sizes[1]), bf16),
            pltpu.VMEM((rows, sizes[0]), bf16),
            pltpu.VMEM((rows, sizes[1]), bf16),
            pltpu.VMEM((rows, max(features, hidden)), bf16),
            pltpu.VMEM((features, width), bf16),
            pltpu.VMEM((owners * mine, width), bf16),
            pltpu.VMEM((rows, width), bf16),
            pltpu.VMEM((rows, width), bf16),
            pltpu.VMEM((rows, hidden), f32),
            pltpu.VMEM((2, mine, width), bf16),
            pltpu.VMEM((mine, width), bf16),
            pltpu.VMEM((most, 1, rows), f32),
            pltpu.VMEM((tallest, rows), f32),
            dma((count,)),
            dma((tall,)),
            dma((tall, deep)),
            dma((count,)),
            dma((3, count)),
            dma((3, 2)),
            dma((3, tall)),
            dma((3, tall, deep)),
            dma((3, count)),
            dma((6,)),
            dma((2, pairs)),
            dma((owners,)),
            dma((2, pairs)),
            dma((2, 2, pairs)),
            dma((2, owners)),
            dma((2, 2, pairs)),
            dma((count, pairs)),
            dma((count, pairs)),
            dma,
            dma,
            dma((2,)),
            dma((2,)),
            pltpu.VMEM((pairs - 1, 2 * mine, width), bf16),
            pltpu.VMEM((counts[0], fulls[0], rows), bf16),
            pltpu.VMEM((counts[1], fulls[1], rows), bf16),
            pltpu.VMEM((latent_size, counts[1] * LANES), bf16),
            pltpu.VMEM((sizes[0], latent_size), bf16),
            pltpu.VMEM((sizes[1], latent_size), bf16),
            pltpu.VMEM((8, LANES), f32),
        ],
        compiler_params=pltpu.CompilerParams(
            collective_id=0, has_side_effects=True, vmem_limit_bytes=67043328
        ),
        cost_estimate=pl.CostEstimate(
            flops=10**11, bytes_accessed=3 * 10**7, transcendentals=2 * 10**7
        ),
    )(
        resid,
        mix_gain,
        out_weight,
        gate_weight,
        up_weight,
        down_weight,
        kv_latent,
        jnp.transpose(rope_key),
        kv_gain,
        turns,
        jnp.transpose(query_large),
        jnp.transpose(query_small),
        up_key_large,
        up_key_small,
        up_value_large,
        up_value_small,
    )


def solution(mesh):
    placed = (
        P(("sp", "tp"), None),
        P("sp", "tp"),
        P("sp", "tp"),
        P("sp", None),
        P("sp", None),
        P(),
        P(None, "tp"),
        P(None, "tp"),
        P(None, "tp"),
        P(None, "tp"),
        P(),
        P(),
        P("sp", "tp"),
        P("sp", "tp"),
        P("sp", "tp"),
    )
    return jax.shard_map(
        functools.partial(on_device, mesh.shape["sp"], mesh.shape["tp"]), mesh=mesh, in_specs=placed, out_specs=P(("sp", "tp"), None), check_vma=False
    )
```

```python
import functools
import math

import jax
import jax.numpy as jnp
from jax import lax
from jax.experimental import pallas as pl
from jax.experimental.pallas import tpu as pltpu
from jax.sharding import PartitionSpec as P

HEADS_SMALL = 8
NOPE_SMALL = 64
NOPE_LARGE = 128
VALUE_SMALL = 64
VALUE_LARGE = 128
ROTARY = 32


THETA = 10000.0
EPSILON = 1e-06
FLOOR = -1e30


LOG2E = math.log2(math.e)
TILE = 256
PAD = 16
LANES = 128
SPIN = NOPE_SMALL


def layer(count, owners, passes, *refs):
    (resid, gain, out_weight) = refs[:3]
    weights = refs[3:6]
    (fresh, spinning, fresh_gain, turns) = refs[6:10]
    asked, raised, valued = refs[10:12], refs[12:14], refs[14:16]
    result = refs[16]
    queries, lifted = refs[-6:-4], refs[-3:-1]
    keyed = tuple(raised[n] if passes[n][0][1] % LANES == 0 else refs[-4] for n in range(2))
    refs = refs[:6] + refs[11:]
    (kv, turned, whole, arrived_a, arrived_b, outs_a, outs_b, joined, projection, resid_all, middle) = refs[12:23]
    (mixer, gated, parts, kept, maxima, sums) = refs[23:29]
    (kv_recv, kv_up, kv_y, kv_d, w_recv, w_z, w_zr, w_y, w_d, own_sem) = refs[29:39]
    (r_send, r_recv, r_pass, a_send, a_recv, a_pass, s_send, s_recv) = refs[39:47]
    (m_send, m_recv, p_send, p_recv, halves) = refs[47:52]
    arrived, outs = (arrived_a, arrived_b), (outs_a, outs_b)

    deep = 1 << ((count.bit_length() - 1) // 2)
    tall = count // deep
    pairs = owners // 2
    blocks = count - 1
    me = lax.axis_index("sp")
    col = lax.axis_index("tp")
    z, y = lax.div(me, deep), lax.rem(me, deep)
    x, core = lax.div(col, 2), lax.rem(col, 2)
    odd = lax.rem(z, 2)
    prime = core == odd
    other = z + 1 - 2 * odd
    token = (z - odd + core) * deep + y
    group = x * 2 + odd
    twin = x * 2 + 1 - core
    rows = fresh.shape[0]
    depth, hidden = weights[0].shape
    mine = resid.shape[0]
    width = resid.shape[1]
    half = rows // 2

    def send(source, target, out_sem, in_sem, sp, tp):
        return pltpu.make_async_remote_copy(
            src_ref=source,
            dst_ref=target,
            send_sem=out_sem,
            recv_sem=in_sem,
            device_id={"sp": sp, "tp": tp},
            device_id_type=pl.DeviceIdType.MESH,
        )

    barrier = pltpu.get_barrier_semaphore()

    def greet(sp, tp):
        pl.semaphore_signal(
            barrier, inc=1, device_id={"sp": sp, "tp": tp}, device_id_type=pl.DeviceIdType.MESH
        )

    for ahead in range(1, tall):
        greet(lax.rem(z + ahead, tall) * deep + y, col)
    for ahead in range(1, deep):
        greet(z * deep + lax.rem(y + ahead, deep), col)
    for ahead in range(1, owners):
        greet(me, lax.rem(col + ahead, owners))
        greet(other * deep + y, lax.rem(col + ahead, owners))
    greet(lax.rem(z - 1 + 2 * odd + tall, tall) * deep + y, twin)
    wide = fresh[...].astype(jnp.float32)
    scaled = wide * lax.rsqrt(jnp.mean(wide * wide, axis=-1, keepdims=True) + EPSILON)
    normed = (scaled * fresh_gain[...].astype(jnp.float32)[None, :]).astype(jnp.bfloat16)
    for part in range(2):
        kv[me, part, :half] = normed[part * half : (part + 1) * half]

    def flipped(values):
        short = -values.shape[1] % LANES
        wide = values.astype(jnp.float32)
        if short:
            wide = jnp.concatenate([wide, jnp.zeros((values.shape[0], short), jnp.float32)], axis=1)
        return wide.T

    def spin(first, second):
        angle_cos, angle_sin = turns[0], turns[1]
        return jnp.concatenate(
            [first * angle_cos - second * angle_sin, second * angle_cos + first * angle_sin], axis=0
        )

    small = ROTARY // 2
    upright = spinning[...].astype(jnp.float32)
    rotated = spin(upright[:small], upright[small:])
    rotated = jnp.concatenate(
        [
            jnp.zeros((SPIN, rows), jnp.float32),
            rotated,
            jnp.zeros((LANES - SPIN - ROTARY, rows), jnp.float32),
        ],
        axis=0,
    ).T.astype(jnp.bfloat16)
    turned[pl.ds(pl.multiple_of(me * rows, rows), rows), :] = rotated
    thick = kv.shape[2] - half
    for part in range(2):
        for piece in range(half // thick):
            at = part * half + piece * thick
            kv[me, part, half:, piece * ROTARY : (piece + 1) * ROTARY] = (
                rotated[at : at + thick, SPIN : SPIN + ROTARY]
            )

    pl.semaphore_wait(barrier, tall - 1 + deep - 1 + 2 * (owners - 1) + 1)

    def latent_up(source, src, away):
        lead = x * 2 + 1 - odd
        return send(source, kv.at[src], kv_up.at[away], kv_recv.at[src], me + deep, lead)

    def latent_over(source, src, away, ahead):
        to = z * deep + lax.rem(y + ahead, deep)
        return send(source, kv.at[src], kv_y.at[away, ahead - 1], kv_recv.at[src], to, col)

    def latent_twin(src):
        return send(kv.at[src], kv.at[src], kv_d.at[src], kv_recv.at[src], me, twin)

    def latent_own(act):
        @pl.when(prime & (z + 1 < tall))
        def _():
            act(latent_up(kv.at[me], me, 0))

        for ahead in range(1, deep):

            @pl.when(jnp.logical_not(prime) & (y + ahead < deep))
            def _():
                act(latent_over(kv.at[me], me, 0, ahead))

    def latent_row(away, act):
        src = me - away * deep

        @pl.when(prime)
        def _():
            @pl.when(z + 1 < tall)
            def _():
                act(latent_up(kv.at[src], src, away))

            act(latent_twin(src))

        @pl.when(jnp.logical_not(prime))
        def _():
            for ahead in range(1, deep):
                act(latent_over(kv.at[src], src, away, ahead))

    def latent_source(step):
        rest = jnp.maximum(step - y - 1, 0)
        spot = lax.rem(rest, deep)
        near = step <= y
        level = jnp.where(near, 0, 1 + lax.div(rest, deep))
        over = jnp.where(near, y - step, lax.rem(y + spot, deep))
        return (z - level) * deep + over, jnp.logical_not(near) & (spot == 0)

    latent_own(lambda copy: copy.start())

    def latent_step(step):
        @pl.when(step <= z)
        def _():
            latent_twin(me - step * deep).wait_recv()
            latent_row(step, lambda copy: copy.start())

        src, straight = latent_source(step)

        @pl.when(jnp.logical_not(straight))
        def _():
            latent_twin(src).wait_recv()

            @pl.when(jnp.logical_not(prime))
            def _():
                latent_twin(src).start()

    def listed(place):
        rising = jnp.where(place - 1 < z, place - 1, place)
        falling = jnp.where(tall - place > z, tall - place, tall - 1 - place)
        return jnp.where(place == 0, z, jnp.where(z < tall // 2, rising, falling))

    def slab(which, src):
        return whole.at[which, pl.ds(pl.multiple_of(src * depth, depth), depth)]

    def weight_z(source, which, src, sem, to):
        return send(source, slab(which, src), sem, w_recv.at[which, src], to * deep + y, col)

    def weight_y(source, which, src, sem, ahead):
        to = z * deep + lax.rem(y + ahead, deep)
        return send(source, slab(which, src), sem, w_recv.at[which, src], to, col)

    def weight_twin(source, which, src, sem):
        return send(source, slab(which, src), sem, w_recv.at[which, src], me, twin)

    def weight_wait(which, src):
        weight_twin(slab(which, src), which, src, w_d.at[which, 0]).wait_recv()

    stride = jnp.where(prime, 2, 1)

    def own_up(which):
        @pl.when(z + stride < tall)
        def _():
            weight_z(weights[which], which, me, w_z.at[which, 0], z + stride).start()

    def own_down(which):
        @pl.when(z - stride >= 0)
        def _():
            weight_z(weights[which], which, me, w_z.at[which, 1], z - stride).start()

    def own_over(which):
        source = weights[which]

        @pl.when(prime)
        def _():
            for ahead in range(1, deep):
                weight_y(source, which, me, w_y.at[which, 0, ahead - 1], ahead).start()
            weight_twin(source, which, me, w_d.at[which, 0]).start()
            pltpu.make_async_copy(source, slab(which, me), own_sem.at[which]).start()

    def place_of(index):
        turn, spot = lax.div(index, deep), lax.rem(index, deep)
        final = turn == tall - 1
        straight = (spot == 0) & (turn < tall - 1)
        place = jnp.where(straight, turn + 1, turn)
        over = jnp.where(straight, 0, jnp.where(final, spot + 1, spot))
        zs = listed(place)
        return straight, place, zs, zs * deep + lax.rem(y + over, deep)

    def relay(which, index):
        straight, place, zs, src = place_of(index)
        weight_wait(which, src)
        block = slab(which, src)

        @pl.when(straight)
        def _():
            @pl.when((zs < z) & (z + 2 < tall))
            def _():
                weight_z(block, which, src, w_zr.at[which, place], z + 2).start()

            @pl.when((zs > z) & (z - 2 >= 0))
            def _():
                weight_z(block, which, src, w_zr.at[which, place], z - 2).start()

            for ahead in range(1, deep):
                weight_y(block, which, src, w_y.at[which, place, ahead - 1], ahead).start()

        weight_twin(block, which, src, w_d.at[which, index + 1]).start()

    def event(number):
        @pl.when(prime & (number == 3))
        def _():
            own_up(1)

        @pl.when(prime & (number == 4))
        def _():
            own_over(2)

        @pl.when(prime & (number == blocks + 3))
        def _():
            own_up(2)
            own_down(2)

        @pl.when(prime & (number < 3 * blocks))
        def _():
            cut = blocks - 3
            mixed = z < tall - 1
            ahead_of = mixed & (number >= cut) & (number < cut + 2)
            behind = mixed & (number >= cut + 2) & (number < blocks + 2)
            which = jnp.where(ahead_of, 1, jnp.where(behind, 0, lax.div(number, blocks)))
            index = jnp.where(ahead_of, number - cut, jnp.where(behind, number - 2, lax.rem(number, blocks)))
            relay(which, index)

    def targets():
        for far in range(2):
            for ahead in range(pairs):
                block = me if far == 0 else other * deep + y
                yield far, ahead, block, lax.rem(x + ahead, pairs) * 2 + odd

    def share(far, ahead, copy):
        if far == 0 and ahead == 0:

            @pl.when(jnp.logical_not(prime))
            def _():
                copy()
        else:
            copy()

    def resid_at(tp):
        return resid_all.at[pl.ds(pl.multiple_of(tp * mine, mine), mine)]

    def resid_sends(act, which):
        for far, ahead, sp, tp in targets():
            if far in which and (far == 0 or ahead == 0):
                share(far, ahead, lambda: act(
                    send(resid, resid_at(col), r_send.at[far, ahead], r_recv.at[col], sp, tp)))

    def resid_passes(act, wait, ranks):
        for rank in ranks:
            side = odd if rank == 0 else 1 - odd
            source = x * 2 + side
            block = resid_at(source)
            if wait:
                send(block, block, r_pass.at[side, 0], r_recv.at[source], me, twin).wait_recv()
            for ahead in range(1, pairs):
                act(send(block, block, r_pass.at[side, ahead], r_recv.at[source],
                         me, lax.rem(x + ahead, pairs) * 2 + core))

    def attn_sends(number, act):
        for far, ahead, sp, tp in targets():
            if far == 0 or ahead == 0:
                share(far, ahead, lambda: act(
                    send(outs[number], arrived[number].at[col], a_send.at[number, far, ahead],
                         a_recv.at[number, col], sp, tp)))

    def attn_passes(number, act, wait):
        for side in range(2):
            source = x * 2 + side
            block = arrived[number].at[source]
            if wait:
                send(block, block, a_pass.at[number, side, 0], a_recv.at[number, source], me, twin).wait_recv()
            for ahead in range(1, pairs):
                act(send(block, block, a_pass.at[number, side, ahead], a_recv.at[number, source],
                         me, lax.rem(x + ahead, pairs) * 2 + core))

    def early_up():
        @pl.when(odd == 0)
        def _():
            resid_sends(lambda copy: copy.start(), (1,))

        own_up(0)

    resid_sends(lambda copy: copy.start(), (0,))
    @pl.when(odd == 1)
    def _():
        resid_sends(lambda copy: copy.start(), (1,))

    own_down(0)
    own_over(0)
    pl.when(jnp.logical_not(prime) & (z > 0))(early_up)

    @pl.when(jnp.logical_not(prime))
    def _():
        own_down(1)

    def first_up():
        pl.when((prime & (odd == 1)) | (z == 0))(early_up)

        @pl.when(jnp.logical_not(prime) & (odd == 1))
        def _():
            own_up(1)

    resid_keep = pltpu.make_async_copy(
        resid, resid_all.at[pl.ds(pl.multiple_of(col * mine, mine), mine)], own_sem.at[4]
    )

    @pl.when(prime)
    def _():
        resid_keep.start()

    projection_keep = pltpu.make_async_copy(out_weight, projection, own_sem.at[5])
    projection_keep.start()

    for number, group in enumerate(passes):
        upright = asked[number]
        tall_values = flipped(valued[number][...])
        for inner, nope, held, size, sum_at in group:
            base = inner * (nope + ROTARY)
            whole_query = queries[number].shape[1]
            gap = whole_query - LANES + SPIN
            queries[number][inner, :nope, :] = upright[base : base + nope, :]
            if gap > nope:
                queries[number][inner, nope:gap, :] = jnp.zeros((gap - nope, rows), jnp.bfloat16)
            queries[number][inner, gap : gap + ROTARY, :] = spin(
                upright[base + nope : base + nope + small, :].astype(jnp.float32),
                upright[base + nope + small : base + nope + ROTARY, :].astype(jnp.float32),
            ).astype(jnp.bfloat16)
            queries[number][inner, gap + ROTARY :, :] = jnp.zeros(
                (whole_query - gap - ROTARY, rows), jnp.bfloat16
            )
            lifted[number][inner * size : (inner + 1) * size, :] = (
                tall_values[inner * size : (inner + 1) * size].astype(jnp.bfloat16)
            )
            if nope % LANES:
                piece = raised[number][:, inner * nope : (inner + 1) * nope]
                blank = jnp.zeros((piece.shape[0], held - nope), jnp.bfloat16)
                keyed[number][:, inner * held : (inner + 1) * held] = jnp.concatenate([piece, blank], axis=1)


    def unpack(index):
        for part in range(2):
            packed = kv[index, part, half:]
            thick = packed.shape[0]
            for piece in range(half // thick):
                slim = packed[:, piece * ROTARY : (piece + 1) * ROTARY]
                before = jnp.zeros((thick, SPIN), jnp.bfloat16)
                after = jnp.zeros((thick, LANES - SPIN - ROTARY), jnp.bfloat16)
                turned[pl.ds(pl.multiple_of(index * rows + part * half + piece * thick, thick), thick), :] = (
                    jnp.concatenate([before, slim, after], axis=1)
                )

    def tiles(number, index, diagonal):
        latent = jnp.concatenate([kv[index, 0, :half], kv[index, 1, :half]], axis=0)
        spun = turned[pl.ds(pl.multiple_of(index * rows, rows), rows), :]
        for head, (inner, nope, held, size, sum_at) in enumerate(passes[number]):
            key = jnp.dot(
                latent, keyed[number][:, inner * held : (inner + 1) * held], preferred_element_type=jnp.float32
            ).astype(jnp.bfloat16)
            key = jnp.concatenate([key, spun], axis=1) if nope % LANES == 0 else key + spun
            value = lax.dot_general(
                lifted[number][inner * size : (inner + 1) * size, :],
                latent,
                (((1,), (1,)), ((), ())),
                preferred_element_type=jnp.float32,
            ).astype(jnp.bfloat16)
            value = jnp.concatenate([value, jnp.ones((PAD, rows), jnp.bfloat16)], axis=0)
            scale = LOG2E / math.sqrt(nope + ROTARY)
            for tile in range(rows // TILE):
                columns = slice(tile * TILE, (tile + 1) * TILE)
                length = (tile + 1) * TILE if diagonal else rows
                scores = jnp.dot(
                    key[:length], queries[number][inner, :, columns], preferred_element_type=jnp.float32
                )
                place = slice(sum_at, sum_at + size + PAD)
                if diagonal:
                    key_pos = lax.broadcasted_iota(jnp.int32, scores.shape, 0)
                    query_pos = lax.broadcasted_iota(jnp.int32, scores.shape, 1) + tile * TILE
                    scores = jnp.where(key_pos <= query_pos, scores, FLOOR)
                    new = jnp.max(scores, axis=0, keepdims=True)
                    weight = jnp.exp2((scores - new) * scale).astype(jnp.bfloat16)
                    maxima[number, head, :, columns] = new
                    sums[number, place, columns] = jnp.dot(
                        value[:, :length], weight, preferred_element_type=jnp.float32
                    )
                else:
                    old = maxima[number, head, :, columns]
                    new = jnp.maximum(old, jnp.max(scores, axis=0, keepdims=True))
                    weight = jnp.exp2((scores - new) * scale).astype(jnp.bfloat16)
                    factor = jnp.exp2((old - new) * scale)
                    maxima[number, head, :, columns] = new
                    sums[number, place, columns] = sums[number, place, columns] * factor + jnp.dot(
                        value, weight, preferred_element_type=jnp.float32
                    )

    def finish(number):
        for inner, nope, held, size, sum_at in passes[number]:
            for tile in range(rows // TILE):
                columns = slice(tile * TILE, (tile + 1) * TILE)
                total = sums[number, sum_at : sum_at + size, columns] / sums[number, sum_at + size : sum_at + size + 1, columns]
                outs[number][columns, inner * size : (inner + 1) * size] = total.T.astype(jnp.bfloat16)
        attn_sends(number, lambda copy: copy.start())

        @pl.when(prime)
        def _():
            arrived[number][col] = outs[number][...]

    tiles(0, me, True)
    tiles(1, me, True)

    def first_step(step, carry):
        latent_step(step)

        pl.when(prime & (odd == 0) & (step == z))(early_up)

        @pl.when(step == 4)
        def _():
            event(0)

        @pl.when(prime & (step == jnp.minimum(me, 4)))
        def _():
            own_down(1)

        src, straight = latent_source(step)
        unpack(src)
        tiles(0, src, False)
        return carry

    lax.fori_loop(1, me + 1, first_step, 0)
    finish(0)

    first_up()
    own_over(1)

    started = jnp.where(me < 4, 1, 0)

    def second_step(step, carry):
        @pl.when(step < 6)
        def _():
            event(step - started)

        for rank in range(2):

            @pl.when(jnp.logical_not(prime) & (step == 1 + 2 * rank))
            def _():
                resid_passes(lambda copy: copy.start(), True, (rank,))

        @pl.when(jnp.logical_not(prime) & (step == 6))
        def _():
            attn_passes(0, lambda copy: copy.start(), True)

        tiles(1, me - step, False)
        return carry

    lax.fori_loop(1, me + 1, second_step, 0)
    finish(1)

    @pl.when(jnp.logical_not(prime))
    def _():
        pl.when(odd == 0)(lambda: own_up(1))

    done = jnp.minimum(me, 5) + 1 - started

    def drain(first, last):
        lax.fori_loop(first, last, lambda number, carry: (event(number), carry)[1], 0)
        return jnp.maximum(first, last)

    done = drain(done, jnp.where(z == tall - 1, done, blocks - 1))

    @pl.when(jnp.logical_not(prime))
    def _():
        for rank in range(2):

            @pl.when(me < 1 + 2 * rank)
            def _():
                resid_passes(lambda copy: copy.start(), True, (rank,))

        @pl.when(me < 6)
        def _():
            attn_passes(0, lambda copy: copy.start(), True)

        attn_passes(1, lambda copy: copy.start(), True)


    @pl.when(jnp.logical_not(prime))
    def _():
        own_up(2)
        own_down(2)


    @pl.when(prime)
    def _():
        resid_keep.wait()

    projection_keep.wait()
    for tp in range(owners):

        @pl.when(jnp.where(prime, tp != col, lax.div(tp, 2) != x))
        def _():
            send(resid, resid_at(tp), r_send.at[0, 0], r_recv.at[tp], me, twin).wait_recv()
            for number in range(2):
                send(outs[number], arrived[number].at[tp], a_send.at[number, 0, 0],
                     a_recv.at[number, tp], me, twin).wait_recv()

        size_a, size_b = outs[0].shape[1], outs[1].shape[1]
        large_from = owners * size_b
        joined[:, tp * size_b : (tp + 1) * size_b] = arrived[1][tp]
        joined[:, large_from + tp * size_a : large_from + (tp + 1) * size_a] = arrived[0][tp]

    features = projection.shape[0]

    def project(part, squares):
        number = done + part

        @pl.when(number < 2 * blocks - 2)
        def _():
            event(number)

        at = pl.ds(pl.multiple_of(part * TILE, TILE), TILE)
        mixed = jnp.dot(joined[:, :features], projection[:, at], preferred_element_type=jnp.float32)
        rounded = (resid_all[:, at].astype(jnp.float32) + mixed).astype(jnp.bfloat16)
        middle[:, at] = rounded
        wide = rounded.astype(jnp.float32)
        return squares + jnp.sum(wide * wide, axis=1, keepdims=True)

    squares = lax.fori_loop(0, width // TILE, project, jnp.zeros((rows, 1), jnp.float32))
    done = jnp.maximum(done, jnp.minimum(done + width // TILE, 2 * blocks - 2))
    scaling = lax.rsqrt(squares * (1.0 / width) + EPSILON)

    def normalise(part, carry):
        at = pl.ds(pl.multiple_of(part * TILE, TILE), TILE)
        scaled = middle[:, at].astype(jnp.float32) * scaling
        mixer[:, at] = (scaled * gain[at].astype(jnp.float32)[None, :]).astype(jnp.bfloat16)
        return carry

    lax.fori_loop(0, width // TILE, normalise, 0)

    def share_middle():
        at = pl.ds(pl.multiple_of(twin * mine, mine), mine)
        return send(middle.at[at], kept, m_send, m_recv, me, twin)

    @pl.when(prime)
    def _():
        share_middle().start()
        kept[...] = middle[pl.ds(pl.multiple_of(col * mine, mine), mine), :]

    def ready(which, first):
        last = drain(first, (which + 1) * blocks + (jnp.where(z < tall - 1, 2, 0) if which == 0 else 0))

        @pl.when(prime)
        def _():
            pltpu.make_async_copy(weights[which], slab(which, me), own_sem.at[which]).wait()

        @pl.when(jnp.logical_not(prime))
        def _():
            lax.fori_loop(0, count, lambda src, carry: (weight_wait(which, src), carry)[1], 0)

        return last

    spans = hidden // TILE

    def over_hidden(body):
        def step(part, carry):
            body(pl.ds(pl.multiple_of(part * TILE, TILE), TILE))
            return carry

        lax.fori_loop(0, spans, step, 0)
        if hidden % TILE:
            body(pl.ds(spans * TILE, hidden % TILE))

    done = ready(0, done)

    def gate_part(at):
        gated[:, at] = jnp.dot(mixer[...], whole[0, :, at], preferred_element_type=jnp.float32)

    over_hidden(gate_part)
    done = ready(1, done)

    def up_part(at):
        value = jnp.dot(mixer[...], whole[1, :, at], preferred_element_type=jnp.float32)
        opened = gated[:, at]
        joined[:, at] = (opened / (1.0 + jnp.exp(-opened)) * value).astype(jnp.bfloat16)

    over_hidden(up_part)
    done = drain(done, 2 * blocks)

    span = 2 * mine

    def columns_of(turn):
        src = jnp.where(turn == 0, me, place_of(jnp.maximum(turn - 1, 0))[3])
        return src, pl.ds(pl.multiple_of(src * depth, depth), depth)

    def row_span(pair):
        return pl.ds(pl.multiple_of(pair * span, span), span)

    def part_swap(turn, ahead):
        to = lax.rem(x + ahead, pairs)
        at = columns_of(turn)[1]
        return send(resid_all.at[row_span(to), at], halves.at[ahead - 1, :, at],
                    s_send.at[turn, ahead - 1], s_recv.at[turn, ahead - 1], me, to * 2 + core)

    def part_send(turn, side):
        at = columns_of(turn)[1]
        rows_at = pl.ds(pl.multiple_of((x * 2 + side) * mine, mine), mine)
        return send(resid_all.at[rows_at, at], parts.at[odd, :, at],
                    p_send.at[side], p_recv.at[odd], token, x * 2 + side)

    def combine(turn):
        at = columns_of(turn)[1]
        total = resid_all[row_span(x), at].astype(jnp.float32)
        for ahead in range(1, pairs):
            part_swap(turn, ahead).wait_recv()
            total = total + halves[ahead - 1, :, at].astype(jnp.float32)
        resid_all[row_span(x), at] = total.astype(jnp.bfloat16)
        for side in range(2):
            local = prime & (side == core)

            @pl.when(jnp.logical_not(local))
            def _():
                part_send(turn, side).start()

            @pl.when(local)
            def _():
                parts[odd, :, at] = total[side * mine : (side + 1) * mine].astype(jnp.bfloat16)

    def lower(turn, carry):
        src, at = columns_of(turn)

        @pl.when(prime & (turn == 0))
        def _():
            pltpu.make_async_copy(weights[2], slab(2, me), own_sem.at[2]).wait()

        @pl.when(prime & (2 * blocks + turn > done))
        def _():
            event(2 * blocks + turn - 1)

        @pl.when(jnp.logical_not(prime))
        def _():
            weight_wait(2, src)

        partial = lax.dot_general(
            joined[:, :hidden], whole[2, at, :], (((1,), (1,)), ((), ())),
            preferred_element_type=jnp.float32,
        ).astype(jnp.bfloat16)
        resid_all[:, at] = partial
        for ahead in range(1, pairs):
            part_swap(turn, ahead).start()

        pl.when(turn > 0)(lambda: combine(turn - 1))
        return carry

    @pl.when(jnp.logical_not(prime))
    def _():
        resid_passes(lambda copy: copy.wait_send(), False, (0, 1))

    lax.fori_loop(0, count, lower, 0)
    combine(count - 1)

    resid_sends(lambda copy: copy.wait_send(), (0, 1))
    for number in range(2):
        attn_sends(number, lambda copy: copy.wait_send())

    @pl.when(jnp.logical_not(prime))
    def _():
        for number in range(2):
            attn_passes(number, lambda copy: copy.wait_send(), False)

    def swap_close(turn, carry):
        for ahead in range(1, pairs):
            part_swap(turn, ahead).wait_send()
        return carry

    lax.fori_loop(0, count, swap_close, 0)
    for side in range(2):
        rows_at = pl.ds(pl.multiple_of((x * 2 + side) * mine, mine), mine)
        copy = send(resid_all.at[rows_at], parts.at[side], p_send.at[side], p_recv.at[side], me, twin)

        @pl.when(jnp.logical_not(prime) | (side != core))
        def _():
            copy.wait_send()

        @pl.when(jnp.logical_not(prime) | (side != odd))
        def _():
            copy.wait_recv()

    @pl.when(prime)
    def _():
        share_middle().wait_send()

    @pl.when(jnp.logical_not(prime))
    def _():
        share_middle().wait_recv()

    total = kept[...].astype(jnp.float32)
    for tp in range(2):
        total = total + parts[tp].astype(jnp.float32)
    result[...] = total.astype(jnp.bfloat16)

    latent_own(lambda copy: copy.wait_send())

    def latent_close(step, carry):
        @pl.when(step <= z)
        def _():
            latent_row(step, lambda copy: copy.wait_send())

        src, straight = latent_source(step)

        @pl.when(jnp.logical_not(straight) & jnp.logical_not(prime))
        def _():
            latent_twin(src).wait_send()

        return carry

    lax.fori_loop(1, me + 1, latent_close, 0)

    def weight_close(which, carry):
        @pl.when(z + stride < tall)
        def _():
            weight_z(slab(which, me), which, me, w_z.at[which, 0], z + stride).wait_send()

        @pl.when(z - stride >= 0)
        def _():
            weight_z(slab(which, me), which, me, w_z.at[which, 1], z - stride).wait_send()

        @pl.when(prime)
        def _():
            for place in range(tall):
                zs = listed(place)

                @pl.when(((zs < z) & (z + 2 < tall)) | ((zs > z) & (z - 2 >= 0)))
                def _():
                    weight_z(slab(which, me), which, me, w_zr.at[which, place], z).wait_send()

                for ahead in range(1, deep):
                    weight_y(slab(which, me), which, me, w_y.at[which, place, ahead - 1], ahead).wait_send()

            for index in range(count):
                weight_twin(slab(which, me), which, me, w_d.at[which, index]).wait_send()

        return carry

    lax.fori_loop(0, 3, weight_close, 0)


def on_device(
    count,
    owners,
    resid,
    query_small,
    query_large,
    kv_latent,
    rope_key,
    kv_gain,
    up_key_small,
    up_value_small,
    up_key_large,
    up_value_large,
    out_weight,
    mix_gain,
    gate_weight,
    up_weight,
    down_weight,
):
    rows, latent_size = kv_latent.shape
    mine, width = resid.shape
    positions = lax.axis_index("sp") * rows + jnp.arange(rows, dtype=jnp.int32)
    inverse = THETA ** (-jnp.arange(0, ROTARY, 2).astype(jnp.float32) / ROTARY)
    phase = inverse[:, None] * positions.astype(jnp.float32)[None, :]
    turns = jnp.stack([jnp.cos(phase), jnp.sin(phase)])
    half = rows // 2
    packed = half + half * ROTARY // latent_size

    passes = []
    for up_key, nope, size in (
        (up_key_large, NOPE_LARGE, VALUE_LARGE),
        (up_key_small, NOPE_SMALL, VALUE_SMALL),
    ):
        held = -(-nope // LANES) * LANES
        passes.append(tuple(
            (head, nope, held, size, head * (size + PAD)) for head in range(up_key.shape[1] // nope)
        ))
    depth, hidden = gate_weight.shape
    features = out_weight.shape[0]
    sizes = [len(group) * group[0][3] for group in passes]
    counts = [len(group) for group in passes]
    fulls = [group[0][1] // LANES * LANES + LANES for group in passes]
    most = max(len(group) for group in passes)
    tallest = max(len(group) * (group[0][3] + PAD) for group in passes)
    deep = 1 << ((count.bit_length() - 1) // 2)
    tall = count // deep
    pairs = owners // 2
    vmem = pl.BlockSpec(memory_space=pltpu.VMEM)
    hbm = pl.BlockSpec(memory_space=pl.ANY)
    bf16, f32 = jnp.bfloat16, jnp.float32
    dma = pltpu.SemaphoreType.DMA
    return pl.pallas_call(
        functools.partial(layer, count, owners, tuple(passes)),
        out_shape=jax.ShapeDtypeStruct((mine, width), bf16),
        in_specs=[hbm, vmem, hbm] + [hbm] * 3 + [vmem] * 10,
        out_specs=vmem,
        scratch_shapes=[
            pltpu.VMEM((count, 2, packed, latent_size), bf16),
            pltpu.VMEM((count * rows, LANES), bf16),
            pltpu.VMEM((3, count * depth, hidden), bf16),
            pltpu.VMEM((owners, rows, sizes[0]), bf16),
            pltpu.VMEM((owners, rows, sizes[1]), bf16),
            pltpu.VMEM((rows, sizes[0]), bf16),
            pltpu.VMEM((rows, sizes[1]), bf16),
            pltpu.VMEM((rows, max(features, hidden)), bf16),
            pltpu.VMEM((features, width), bf16),
            pltpu.VMEM((owners * mine, width), bf16),
            pltpu.VMEM((rows, width), bf16),
            pltpu.VMEM((rows, width), bf16),
            pltpu.VMEM((rows, hidden), f32),
            pltpu.VMEM((2, mine, width), bf16),
            pltpu.VMEM((mine, width), bf16),
            pltpu.VMEM((2, most, 1, rows), f32),
            pltpu.VMEM((2, tallest, rows), f32),
            dma((count,)),
            dma((tall,)),
            dma((tall, deep)),
            dma((count,)),
            dma((3, count)),
            dma((3, 2)),
            dma((3, tall)),
            dma((3, tall, deep)),
            dma((3, count)),
            dma((6,)),
            dma((2, pairs)),
            dma((owners,)),
            dma((2, pairs)),
            dma((2, 2, pairs)),
            dma((2, owners)),
            dma((2, 2, pairs)),
            dma((count, pairs)),
            dma((count, pairs)),
            dma,
            dma,
            dma((2,)),
            dma((2,)),
            pltpu.VMEM((pairs - 1, 2 * mine, width), bf16),
            pltpu.VMEM((counts[0], fulls[0], rows), bf16),
            pltpu.VMEM((counts[1], fulls[1], rows), bf16),
            pltpu.VMEM((latent_size, counts[1] * LANES), bf16),
            pltpu.VMEM((sizes[0], latent_size), bf16),
            pltpu.VMEM((sizes[1], latent_size), bf16),
            pltpu.VMEM((8, LANES), f32),
        ],
        compiler_params=pltpu.CompilerParams(
            collective_id=0, has_side_effects=True, vmem_limit_bytes=67043328
        ),
        cost_estimate=pl.CostEstimate(
            flops=10**11, bytes_accessed=3 * 10**7, transcendentals=2 * 10**7
        ),
    )(
        resid,
        mix_gain,
        out_weight,
        gate_weight,
        up_weight,
        down_weight,
        kv_latent,
        jnp.transpose(rope_key),
        kv_gain,
        turns,
        jnp.transpose(query_large),
        jnp.transpose(query_small),
        up_key_large,
        up_key_small,
        up_value_large,
        up_value_small,
    )


def solution(mesh):
    placed = (
        P(("sp", "tp"), None),
        P("sp", "tp"),
        P("sp", "tp"),
        P("sp", None),
        P("sp", None),
        P(),
        P(None, "tp"),
        P(None, "tp"),
        P(None, "tp"),
        P(None, "tp"),
        P(),
        P(),
        P("sp", "tp"),
        P("sp", "tp"),
        P("sp", "tp"),
    )
    return jax.shard_map(
        functools.partial(on_device, mesh.shape["sp"], mesh.shape["tp"]), mesh=mesh, in_specs=placed, out_specs=P(("sp", "tp"), None), check_vma=False
    )
```

```python
import functools
import math

import jax
import jax.numpy as jnp
from jax import lax
from jax.experimental import pallas as pl
from jax.experimental.pallas import tpu as pltpu
from jax.sharding import PartitionSpec as P

HEADS_SMALL = 8
NOPE_SMALL = 64
NOPE_LARGE = 128
VALUE_SMALL = 64
VALUE_LARGE = 128
ROTARY = 32


THETA = 10000.0
EPSILON = 1e-06
FLOOR = -1e30


LOG2E = math.log2(math.e)
TILE = 256
BROAD = 512
PAD = 16
LANES = 128
SPIN = NOPE_SMALL


def layer(count, owners, passes, *refs):
    (resid, gain, out_weight) = refs[:3]
    weights = refs[3:6]
    (fresh, spinning, fresh_gain, turns) = refs[6:10]
    asked, raised, valued = refs[10:12], refs[12:14], refs[14:16]
    result = refs[16]
    queries, lifted = refs[-6:-4], refs[-3:-1]
    keyed = tuple(raised[n] if passes[n][0][1] % LANES == 0 else refs[-4] for n in range(2))
    refs = refs[:6] + refs[11:]
    (kv, turned, whole, arrived_a, arrived_b, outs_a, outs_b, joined, projection, resid_all, middle) = refs[12:23]
    (mixer, gated, parts, kept, maxima, sums) = refs[23:29]
    (kv_recv, kv_up, kv_y, kv_d, w_recv, w_z, w_zr, w_y, w_d, own_sem) = refs[29:39]
    (r_send, r_recv, r_pass, a_send, a_recv, a_pass, s_send, s_recv) = refs[39:47]
    (m_send, m_recv, p_send, p_recv, halves) = refs[47:52]
    arrived, outs = (arrived_a, arrived_b), (outs_a, outs_b)

    deep = 1 << ((count.bit_length() - 1) // 2)
    tall = count // deep
    pairs = owners // 2
    blocks = count - 1
    me = lax.axis_index("sp")
    col = lax.axis_index("tp")
    z, y = lax.div(me, deep), lax.rem(me, deep)
    x, core = lax.div(col, 2), lax.rem(col, 2)
    odd = lax.rem(z, 2)
    prime = core == odd
    other = z + 1 - 2 * odd
    token = (z - odd + core) * deep + y
    group = x * 2 + odd
    twin = x * 2 + 1 - core
    rows = fresh.shape[0]
    depth, hidden = weights[0].shape
    mine = resid.shape[0]
    width = resid.shape[1]
    half = rows // 2

    def send(source, target, out_sem, in_sem, sp, tp):
        return pltpu.make_async_remote_copy(
            src_ref=source,
            dst_ref=target,
            send_sem=out_sem,
            recv_sem=in_sem,
            device_id={"sp": sp, "tp": tp},
            device_id_type=pl.DeviceIdType.MESH,
        )

    barrier = pltpu.get_barrier_semaphore()

    def greet(sp, tp):
        pl.semaphore_signal(
            barrier, inc=1, device_id={"sp": sp, "tp": tp}, device_id_type=pl.DeviceIdType.MESH
        )

    for ahead in range(1, tall):
        greet(lax.rem(z + ahead, tall) * deep + y, col)
    for ahead in range(1, deep):
        greet(z * deep + lax.rem(y + ahead, deep), col)
    for ahead in range(1, owners):
        greet(me, lax.rem(col + ahead, owners))
        greet(other * deep + y, lax.rem(col + ahead, owners))
    greet(lax.rem(z - 1 + 2 * odd + tall, tall) * deep + y, twin)
    wide = fresh[...].astype(jnp.float32)
    scaled = wide * lax.rsqrt(jnp.mean(wide * wide, axis=-1, keepdims=True) + EPSILON)
    normed = (scaled * fresh_gain[...].astype(jnp.float32)[None, :]).astype(jnp.bfloat16)
    for part in range(2):
        kv[me, part, :half] = normed[part * half : (part + 1) * half]

    def flipped(values):
        short = -values.shape[1] % LANES
        wide = values.astype(jnp.float32)
        if short:
            wide = jnp.concatenate([wide, jnp.zeros((values.shape[0], short), jnp.float32)], axis=1)
        return wide.T

    def spin(first, second):
        angle_cos, angle_sin = turns[0], turns[1]
        return jnp.concatenate(
            [first * angle_cos - second * angle_sin, second * angle_cos + first * angle_sin], axis=0
        )

    small = ROTARY // 2
    upright = spinning[...].astype(jnp.float32)
    rotated = spin(upright[:small], upright[small:])
    rotated = jnp.concatenate(
        [
            jnp.zeros((SPIN, rows), jnp.float32),
            rotated,
            jnp.zeros((LANES - SPIN - ROTARY, rows), jnp.float32),
        ],
        axis=0,
    ).T.astype(jnp.bfloat16)
    turned[pl.ds(pl.multiple_of(me * rows, rows), rows), :] = rotated
    thick = kv.shape[2] - half
    for part in range(2):
        for piece in range(half // thick):
            at = part * half + piece * thick
            kv[me, part, half:, piece * ROTARY : (piece + 1) * ROTARY] = (
                rotated[at : at + thick, SPIN : SPIN + ROTARY]
            )

    pl.semaphore_wait(barrier, tall - 1 + deep - 1 + 2 * (owners - 1) + 1)

    def latent_up(source, src, away):
        lead = x * 2 + 1 - odd
        return send(source, kv.at[src], kv_up.at[away], kv_recv.at[src], me + deep, lead)

    def latent_over(source, src, away, ahead):
        to = z * deep + lax.rem(y + ahead, deep)
        return send(source, kv.at[src], kv_y.at[away, ahead - 1], kv_recv.at[src], to, col)

    def latent_twin(src):
        return send(kv.at[src], kv.at[src], kv_d.at[src], kv_recv.at[src], me, twin)

    def latent_own(act):
        @pl.when(prime & (z + 1 < tall))
        def _():
            act(latent_up(kv.at[me], me, 0))

        for ahead in range(1, deep):

            @pl.when(jnp.logical_not(prime) & (y + ahead < deep))
            def _():
                act(latent_over(kv.at[me], me, 0, ahead))

    def latent_row(away, act):
        src = me - away * deep

        @pl.when(prime)
        def _():
            @pl.when(z + 1 < tall)
            def _():
                act(latent_up(kv.at[src], src, away))

            act(latent_twin(src))

        @pl.when(jnp.logical_not(prime))
        def _():
            for ahead in range(1, deep):
                act(latent_over(kv.at[src], src, away, ahead))

    def latent_source(step):
        rest = jnp.maximum(step - y - 1, 0)
        spot = lax.rem(rest, deep)
        near = step <= y
        level = jnp.where(near, 0, 1 + lax.div(rest, deep))
        over = jnp.where(near, y - step, lax.rem(y + spot, deep))
        return (z - level) * deep + over, jnp.logical_not(near) & (spot == 0)

    latent_own(lambda copy: copy.start())

    def latent_step(step):
        @pl.when(step <= z)
        def _():
            latent_twin(me - step * deep).wait_recv()
            latent_row(step, lambda copy: copy.start())

        src, straight = latent_source(step)

        @pl.when(jnp.logical_not(straight))
        def _():
            latent_twin(src).wait_recv()

            @pl.when(jnp.logical_not(prime))
            def _():
                latent_twin(src).start()

    def listed(place):
        rising = jnp.where(place - 1 < z, place - 1, place)
        falling = jnp.where(tall - place > z, tall - place, tall - 1 - place)
        return jnp.where(place == 0, z, jnp.where(z < tall // 2, rising, falling))

    def slab(which, src):
        return whole.at[which, pl.ds(pl.multiple_of(src * depth, depth), depth)]

    def weight_z(source, which, src, sem, to):
        return send(source, slab(which, src), sem, w_recv.at[which, src], to * deep + y, col)

    def weight_y(source, which, src, sem, ahead):
        to = z * deep + lax.rem(y + ahead, deep)
        return send(source, slab(which, src), sem, w_recv.at[which, src], to, col)

    def weight_twin(source, which, src, sem):
        return send(source, slab(which, src), sem, w_recv.at[which, src], me, twin)

    def weight_wait(which, src):
        weight_twin(slab(which, src), which, src, w_d.at[which, 0]).wait_recv()

    stride = jnp.where(prime, 2, 1)

    def own_up(which):
        @pl.when(z + stride < tall)
        def _():
            weight_z(weights[which], which, me, w_z.at[which, 0], z + stride).start()

    def own_down(which):
        @pl.when(z - stride >= 0)
        def _():
            weight_z(weights[which], which, me, w_z.at[which, 1], z - stride).start()

    def own_over(which):
        source = weights[which]

        @pl.when(prime)
        def _():
            for ahead in range(1, deep):
                weight_y(source, which, me, w_y.at[which, 0, ahead - 1], ahead).start()
            weight_twin(source, which, me, w_d.at[which, 0]).start()
            pltpu.make_async_copy(source, slab(which, me), own_sem.at[which]).start()

    def place_of(index):
        turn, spot = lax.div(index, deep), lax.rem(index, deep)
        final = turn == tall - 1
        straight = (spot == 0) & (turn < tall - 1)
        place = jnp.where(straight, turn + 1, turn)
        over = jnp.where(straight, 0, jnp.where(final, spot + 1, spot))
        zs = listed(place)
        return straight, place, zs, zs * deep + lax.rem(y + over, deep)

    def relay(which, index):
        straight, place, zs, src = place_of(index)
        weight_wait(which, src)
        block = slab(which, src)

        @pl.when(straight)
        def _():
            @pl.when((zs < z) & (z + 2 < tall))
            def _():
                weight_z(block, which, src, w_zr.at[which, place], z + 2).start()

            @pl.when((zs > z) & (z - 2 >= 0))
            def _():
                weight_z(block, which, src, w_zr.at[which, place], z - 2).start()

            for ahead in range(1, deep):
                weight_y(block, which, src, w_y.at[which, place, ahead - 1], ahead).start()

        weight_twin(block, which, src, w_d.at[which, index + 1]).start()

    def event(number):
        @pl.when(prime & (number == 3))
        def _():
            own_up(1)

        @pl.when(prime & (number == 4))
        def _():
            own_over(2)

        @pl.when(prime & (number == blocks + 3))
        def _():
            own_up(2)
            own_down(2)

        @pl.when(prime & (number < 3 * blocks))
        def _():
            cut = blocks - 3
            mixed = z < tall - 1
            ahead_of = mixed & (number >= cut) & (number < cut + 2)
            behind = mixed & (number >= cut + 2) & (number < blocks + 2)
            which = jnp.where(ahead_of, 1, jnp.where(behind, 0, lax.div(number, blocks)))
            index = jnp.where(ahead_of, number - cut, jnp.where(behind, number - 2, lax.rem(number, blocks)))
            relay(which, index)

    def targets():
        for far in range(2):
            for ahead in range(pairs):
                block = me if far == 0 else other * deep + y
                yield far, ahead, block, lax.rem(x + ahead, pairs) * 2 + odd

    def share(far, ahead, copy):
        if far == 0 and ahead == 0:

            @pl.when(jnp.logical_not(prime))
            def _():
                copy()
        else:
            copy()

    def resid_at(tp):
        return resid_all.at[pl.ds(pl.multiple_of(tp * mine, mine), mine)]

    def resid_sends(act, which):
        for far, ahead, sp, tp in targets():
            if far in which and (far == 0 or ahead == 0):
                share(far, ahead, lambda: act(
                    send(resid, resid_at(col), r_send.at[far, ahead], r_recv.at[col], sp, tp)))

    def resid_passes(act, wait, ranks):
        for rank in ranks:
            side = odd if rank == 0 else 1 - odd
            source = x * 2 + side
            block = resid_at(source)
            if wait:
                send(block, block, r_pass.at[side, 0], r_recv.at[source], me, twin).wait_recv()
            for ahead in range(1, pairs):
                act(send(block, block, r_pass.at[side, ahead], r_recv.at[source],
                         me, lax.rem(x + ahead, pairs) * 2 + core))

    def attn_sends(number, act):
        for far, ahead, sp, tp in targets():
            if far == 0 or ahead == 0:
                share(far, ahead, lambda: act(
                    send(outs[number], arrived[number].at[col], a_send.at[number, far, ahead],
                         a_recv.at[number, col], sp, tp)))

    def attn_passes(number, act, wait):
        for side in range(2):
            source = x * 2 + side
            block = arrived[number].at[source]
            if wait:
                send(block, block, a_pass.at[number, side, 0], a_recv.at[number, source], me, twin).wait_recv()
            for ahead in range(1, pairs):
                act(send(block, block, a_pass.at[number, side, ahead], a_recv.at[number, source],
                         me, lax.rem(x + ahead, pairs) * 2 + core))

    def early_up():
        @pl.when(odd == 0)
        def _():
            resid_sends(lambda copy: copy.start(), (1,))

        own_up(0)

    resid_sends(lambda copy: copy.start(), (0,))
    @pl.when(odd == 1)
    def _():
        resid_sends(lambda copy: copy.start(), (1,))

    own_down(0)
    own_over(0)
    pl.when(jnp.logical_not(prime) & (z > 0))(early_up)

    @pl.when(jnp.logical_not(prime))
    def _():
        own_down(1)

    def first_up():
        pl.when((prime & (odd == 1)) | (z == 0))(early_up)

        @pl.when(jnp.logical_not(prime) & (odd == 1))
        def _():
            own_up(1)

    resid_keep = pltpu.make_async_copy(
        resid, resid_all.at[pl.ds(pl.multiple_of(col * mine, mine), mine)], own_sem.at[4]
    )

    @pl.when(prime)
    def _():
        resid_keep.start()

    projection_keep = pltpu.make_async_copy(out_weight, projection, own_sem.at[5])
    projection_keep.start()

    for number, group in enumerate(passes):
        upright = asked[number]
        tall_values = flipped(valued[number][...])
        for inner, nope, held, size, sum_at in group:
            base = inner * (nope + ROTARY)
            whole_query = queries[number].shape[1]
            gap = whole_query - LANES + SPIN
            queries[number][inner, :nope, :] = upright[base : base + nope, :]
            if gap > nope:
                queries[number][inner, nope:gap, :] = jnp.zeros((gap - nope, rows), jnp.bfloat16)
            queries[number][inner, gap : gap + ROTARY, :] = spin(
                upright[base + nope : base + nope + small, :].astype(jnp.float32),
                upright[base + nope + small : base + nope + ROTARY, :].astype(jnp.float32),
            ).astype(jnp.bfloat16)
            queries[number][inner, gap + ROTARY :, :] = jnp.zeros(
                (whole_query - gap - ROTARY, rows), jnp.bfloat16
            )
            lifted[number][inner * size : (inner + 1) * size, :] = (
                tall_values[inner * size : (inner + 1) * size].astype(jnp.bfloat16)
            )
            if nope % LANES:
                piece = raised[number][:, inner * nope : (inner + 1) * nope]
                blank = jnp.zeros((piece.shape[0], held - nope), jnp.bfloat16)
                keyed[number][:, inner * held : (inner + 1) * held] = jnp.concatenate([piece, blank], axis=1)


    def unpack(index):
        for part in range(2):
            packed = kv[index, part, half:]
            thick = packed.shape[0]
            for piece in range(half // thick):
                slim = packed[:, piece * ROTARY : (piece + 1) * ROTARY]
                before = jnp.zeros((thick, SPIN), jnp.bfloat16)
                after = jnp.zeros((thick, LANES - SPIN - ROTARY), jnp.bfloat16)
                turned[pl.ds(pl.multiple_of(index * rows + part * half + piece * thick, thick), thick), :] = (
                    jnp.concatenate([before, slim, after], axis=1)
                )

    def tiles(number, index, diagonal):
        latent = jnp.concatenate([kv[index, 0, :half], kv[index, 1, :half]], axis=0)
        spun = turned[pl.ds(pl.multiple_of(index * rows, rows), rows), :]
        for head, (inner, nope, held, size, sum_at) in enumerate(passes[number]):
            key = jnp.dot(
                latent, keyed[number][:, inner * held : (inner + 1) * held], preferred_element_type=jnp.float32
            ).astype(jnp.bfloat16)
            key = jnp.concatenate([key, spun], axis=1) if nope % LANES == 0 else key + spun
            value = lax.dot_general(
                lifted[number][inner * size : (inner + 1) * size, :],
                latent,
                (((1,), (1,)), ((), ())),
                preferred_element_type=jnp.float32,
            ).astype(jnp.bfloat16)
            value = jnp.concatenate([value, jnp.ones((PAD, rows), jnp.bfloat16)], axis=0)
            scale = LOG2E / math.sqrt(nope + ROTARY)
            for tile in range(rows // TILE):
                columns = slice(tile * TILE, (tile + 1) * TILE)
                length = (tile + 1) * TILE if diagonal else rows
                scores = jnp.dot(
                    key[:length], queries[number][inner, :, columns], preferred_element_type=jnp.float32
                )
                place = slice(sum_at, sum_at + size + PAD)
                if diagonal:
                    key_pos = lax.broadcasted_iota(jnp.int32, scores.shape, 0)
                    query_pos = lax.broadcasted_iota(jnp.int32, scores.shape, 1) + tile * TILE
                    scores = jnp.where(key_pos <= query_pos, scores, FLOOR)
                    new = jnp.max(scores, axis=0, keepdims=True)
                    weight = jnp.exp2((scores - new) * scale).astype(jnp.bfloat16)
                    maxima[number, head, :, columns] = new
                    sums[number, place, columns] = jnp.dot(
                        value[:, :length], weight, preferred_element_type=jnp.float32
                    )
                else:
                    old = maxima[number, head, :, columns]
                    new = jnp.maximum(old, jnp.max(scores, axis=0, keepdims=True))
                    weight = jnp.exp2((scores - new) * scale).astype(jnp.bfloat16)
                    factor = jnp.exp2((old - new) * scale)
                    maxima[number, head, :, columns] = new
                    sums[number, place, columns] = sums[number, place, columns] * factor + jnp.dot(
                        value, weight, preferred_element_type=jnp.float32
                    )

    def finish(number):
        for inner, nope, held, size, sum_at in passes[number]:
            for tile in range(rows // TILE):
                columns = slice(tile * TILE, (tile + 1) * TILE)
                total = sums[number, sum_at : sum_at + size, columns] / sums[number, sum_at + size : sum_at + size + 1, columns]
                outs[number][columns, inner * size : (inner + 1) * size] = total.T.astype(jnp.bfloat16)
        attn_sends(number, lambda copy: copy.start())

        @pl.when(prime)
        def _():
            arrived[number][col] = outs[number][...]

    tiles(0, me, True)
    tiles(1, me, True)

    def first_step(step, carry):
        latent_step(step)

        pl.when(prime & (odd == 0) & (step == z))(early_up)

        @pl.when(step == 4)
        def _():
            event(0)

        @pl.when(prime & (step == jnp.minimum(me, 4)))
        def _():
            own_down(1)

        src, straight = latent_source(step)
        unpack(src)
        tiles(0, src, False)
        return carry

    lax.fori_loop(1, me + 1, first_step, 0)
    finish(0)

    first_up()
    own_over(1)

    started = jnp.where(me < 4, 1, 0)

    def second_step(step, carry):
        @pl.when(step < 6)
        def _():
            event(step - started)

        for rank in range(2):

            @pl.when(jnp.logical_not(prime) & (step == 1 + 2 * rank))
            def _():
                resid_passes(lambda copy: copy.start(), True, (rank,))

        @pl.when(jnp.logical_not(prime) & (step == 6))
        def _():
            attn_passes(0, lambda copy: copy.start(), True)

        tiles(1, me - step, False)
        return carry

    lax.fori_loop(1, me + 1, second_step, 0)
    finish(1)

    @pl.when(jnp.logical_not(prime))
    def _():
        pl.when(odd == 0)(lambda: own_up(1))

    done = jnp.minimum(me, 5) + 1 - started

    def drain(first, last):
        lax.fori_loop(first, last, lambda number, carry: (event(number), carry)[1], 0)
        return jnp.maximum(first, last)

    done = drain(done, jnp.where(z == tall - 1, done, blocks - 1))

    @pl.when(jnp.logical_not(prime))
    def _():
        for rank in range(2):

            @pl.when(me < 1 + 2 * rank)
            def _():
                resid_passes(lambda copy: copy.start(), True, (rank,))

        @pl.when(me < 6)
        def _():
            attn_passes(0, lambda copy: copy.start(), True)

        attn_passes(1, lambda copy: copy.start(), True)


    @pl.when(jnp.logical_not(prime))
    def _():
        own_up(2)
        own_down(2)


    @pl.when(prime)
    def _():
        resid_keep.wait()

    projection_keep.wait()
    for tp in range(owners):

        @pl.when(jnp.where(prime, tp != col, lax.div(tp, 2) != x))
        def _():
            send(resid, resid_at(tp), r_send.at[0, 0], r_recv.at[tp], me, twin).wait_recv()
            for number in range(2):
                send(outs[number], arrived[number].at[tp], a_send.at[number, 0, 0],
                     a_recv.at[number, tp], me, twin).wait_recv()

        size_a, size_b = outs[0].shape[1], outs[1].shape[1]
        large_from = owners * size_b
        joined[:, tp * size_b : (tp + 1) * size_b] = arrived[1][tp]
        joined[:, large_from + tp * size_a : large_from + (tp + 1) * size_a] = arrived[0][tp]

    features = projection.shape[0]

    def project(part, squares):
        number = done + part

        @pl.when(number < 2 * blocks - 2)
        def _():
            event(number)

        at = pl.ds(pl.multiple_of(part * TILE, TILE), TILE)
        mixed = jnp.dot(joined[:, :features], projection[:, at], preferred_element_type=jnp.float32)
        rounded = (resid_all[:, at].astype(jnp.float32) + mixed).astype(jnp.bfloat16)
        middle[:, at] = rounded
        wide = rounded.astype(jnp.float32)
        return squares + jnp.sum(wide * wide, axis=1, keepdims=True)

    squares = lax.fori_loop(0, width // TILE, project, jnp.zeros((rows, 1), jnp.float32))
    done = jnp.maximum(done, jnp.minimum(done + width // TILE, 2 * blocks - 2))
    scaling = lax.rsqrt(squares * (1.0 / width) + EPSILON)

    def normalise(part, carry):
        at = pl.ds(pl.multiple_of(part * TILE, TILE), TILE)
        scaled = middle[:, at].astype(jnp.float32) * scaling
        mixer[:, at] = (scaled * gain[at].astype(jnp.float32)[None, :]).astype(jnp.bfloat16)
        return carry

    lax.fori_loop(0, width // TILE, normalise, 0)

    def share_middle():
        at = pl.ds(pl.multiple_of(twin * mine, mine), mine)
        return send(middle.at[at], kept, m_send, m_recv, me, twin)

    @pl.when(prime)
    def _():
        share_middle().start()
        kept[...] = middle[pl.ds(pl.multiple_of(col * mine, mine), mine), :]

    def ready(which, first):
        last = drain(first, (which + 1) * blocks + (jnp.where(z < tall - 1, 2, 0) if which == 0 else 0))

        @pl.when(prime)
        def _():
            pltpu.make_async_copy(weights[which], slab(which, me), own_sem.at[which]).wait()

        @pl.when(jnp.logical_not(prime))
        def _():
            lax.fori_loop(0, count, lambda src, carry: (weight_wait(which, src), carry)[1], 0)

        return last

    spans = hidden // BROAD

    def over_hidden(body):
        def step(part, carry):
            body(pl.ds(pl.multiple_of(part * BROAD, BROAD), BROAD))
            return carry

        lax.fori_loop(0, spans, step, 0)
        if hidden % BROAD:
            body(pl.ds(spans * BROAD, hidden % BROAD))

    done = ready(0, done)

    def gate_part(at):
        gated[:, at] = jnp.dot(mixer[...], whole[0, :, at], preferred_element_type=jnp.float32)

    over_hidden(gate_part)
    done = ready(1, done)

    def up_part(at):
        value = jnp.dot(mixer[...], whole[1, :, at], preferred_element_type=jnp.float32)
        opened = gated[:, at]
        joined[:, at] = (opened / (1.0 + jnp.exp(-opened)) * value).astype(jnp.bfloat16)

    over_hidden(up_part)
    done = drain(done, 2 * blocks)

    span = 2 * mine

    def columns_of(turn):
        src = jnp.where(turn == 0, me, place_of(jnp.maximum(turn - 1, 0))[3])
        return src, pl.ds(pl.multiple_of(src * depth, depth), depth)

    def row_span(pair):
        return pl.ds(pl.multiple_of(pair * span, span), span)

    def part_swap(turn, ahead):
        to = lax.rem(x + ahead, pairs)
        at = columns_of(turn)[1]
        return send(resid_all.at[row_span(to), at], halves.at[ahead - 1, :, at],
                    s_send.at[turn, ahead - 1], s_recv.at[turn, ahead - 1], me, to * 2 + core)

    def part_send(turn, side):
        at = columns_of(turn)[1]
        rows_at = pl.ds(pl.multiple_of((x * 2 + side) * mine, mine), mine)
        return send(resid_all.at[rows_at, at], parts.at[odd, :, at],
                    p_send.at[side], p_recv.at[odd], token, x * 2 + side)

    def combine(turn):
        at = columns_of(turn)[1]
        total = resid_all[row_span(x), at].astype(jnp.float32)
        for ahead in range(1, pairs):
            part_swap(turn, ahead).wait_recv()
            total = total + halves[ahead - 1, :, at].astype(jnp.float32)
        resid_all[row_span(x), at] = total.astype(jnp.bfloat16)
        for side in range(2):
            local = prime & (side == core)

            @pl.when(jnp.logical_not(local))
            def _():
                part_send(turn, side).start()

            @pl.when(local)
            def _():
                parts[odd, :, at] = total[side * mine : (side + 1) * mine].astype(jnp.bfloat16)

    def lower(turn, carry):
        src, at = columns_of(turn)

        @pl.when(prime & (turn == 0))
        def _():
            pltpu.make_async_copy(weights[2], slab(2, me), own_sem.at[2]).wait()

        @pl.when(prime & (2 * blocks + turn > done))
        def _():
            event(2 * blocks + turn - 1)

        @pl.when(jnp.logical_not(prime))
        def _():
            weight_wait(2, src)

        partial = lax.dot_general(
            joined[:, :hidden], whole[2, at, :], (((1,), (1,)), ((), ())),
            preferred_element_type=jnp.float32,
        ).astype(jnp.bfloat16)
        resid_all[:, at] = partial
        for ahead in range(1, pairs):
            part_swap(turn, ahead).start()

        pl.when(turn > 0)(lambda: combine(turn - 1))
        return carry

    @pl.when(jnp.logical_not(prime))
    def _():
        resid_passes(lambda copy: copy.wait_send(), False, (0, 1))

    lax.fori_loop(0, count, lower, 0)
    combine(count - 1)

    resid_sends(lambda copy: copy.wait_send(), (0, 1))
    for number in range(2):
        attn_sends(number, lambda copy: copy.wait_send())

    @pl.when(jnp.logical_not(prime))
    def _():
        for number in range(2):
            attn_passes(number, lambda copy: copy.wait_send(), False)

    def swap_close(turn, carry):
        for ahead in range(1, pairs):
            part_swap(turn, ahead).wait_send()
        return carry

    lax.fori_loop(0, count, swap_close, 0)
    for side in range(2):
        rows_at = pl.ds(pl.multiple_of((x * 2 + side) * mine, mine), mine)
        copy = send(resid_all.at[rows_at], parts.at[side], p_send.at[side], p_recv.at[side], me, twin)

        @pl.when(jnp.logical_not(prime) | (side != core))
        def _():
            copy.wait_send()

        @pl.when(jnp.logical_not(prime) | (side != odd))
        def _():
            copy.wait_recv()

    @pl.when(prime)
    def _():
        share_middle().wait_send()

    @pl.when(jnp.logical_not(prime))
    def _():
        share_middle().wait_recv()

    total = kept[...].astype(jnp.float32)
    for tp in range(2):
        total = total + parts[tp].astype(jnp.float32)
    result[...] = total.astype(jnp.bfloat16)

    latent_own(lambda copy: copy.wait_send())

    def latent_close(step, carry):
        @pl.when(step <= z)
        def _():
            latent_row(step, lambda copy: copy.wait_send())

        src, straight = latent_source(step)

        @pl.when(jnp.logical_not(straight) & jnp.logical_not(prime))
        def _():
            latent_twin(src).wait_send()

        return carry

    lax.fori_loop(1, me + 1, latent_close, 0)

    def weight_close(which, carry):
        @pl.when(z + stride < tall)
        def _():
            weight_z(slab(which, me), which, me, w_z.at[which, 0], z + stride).wait_send()

        @pl.when(z - stride >= 0)
        def _():
            weight_z(slab(which, me), which, me, w_z.at[which, 1], z - stride).wait_send()

        @pl.when(prime)
        def _():
            for place in range(tall):
                zs = listed(place)

                @pl.when(((zs < z) & (z + 2 < tall)) | ((zs > z) & (z - 2 >= 0)))
                def _():
                    weight_z(slab(which, me), which, me, w_zr.at[which, place], z).wait_send()

                for ahead in range(1, deep):
                    weight_y(slab(which, me), which, me, w_y.at[which, place, ahead - 1], ahead).wait_send()

            for index in range(count):
                weight_twin(slab(which, me), which, me, w_d.at[which, index]).wait_send()

        return carry

    lax.fori_loop(0, 3, weight_close, 0)


def on_device(
    count,
    owners,
    resid,
    query_small,
    query_large,
    kv_latent,
    rope_key,
    kv_gain,
    up_key_small,
    up_value_small,
    up_key_large,
    up_value_large,
    out_weight,
    mix_gain,
    gate_weight,
    up_weight,
    down_weight,
):
    rows, latent_size = kv_latent.shape
    mine, width = resid.shape
    positions = lax.axis_index("sp") * rows + jnp.arange(rows, dtype=jnp.int32)
    inverse = THETA ** (-jnp.arange(0, ROTARY, 2).astype(jnp.float32) / ROTARY)
    phase = inverse[:, None] * positions.astype(jnp.float32)[None, :]
    turns = jnp.stack([jnp.cos(phase), jnp.sin(phase)])
    half = rows // 2
    packed = half + half * ROTARY // latent_size

    passes = []
    for up_key, nope, size in (
        (up_key_large, NOPE_LARGE, VALUE_LARGE),
        (up_key_small, NOPE_SMALL, VALUE_SMALL),
    ):
        held = -(-nope // LANES) * LANES
        passes.append(tuple(
            (head, nope, held, size, head * (size + PAD)) for head in range(up_key.shape[1] // nope)
        ))
    depth, hidden = gate_weight.shape
    features = out_weight.shape[0]
    sizes = [len(group) * group[0][3] for group in passes]
    counts = [len(group) for group in passes]
    fulls = [group[0][1] // LANES * LANES + LANES for group in passes]
    most = max(len(group) for group in passes)
    tallest = max(len(group) * (group[0][3] + PAD) for group in passes)
    deep = 1 << ((count.bit_length() - 1) // 2)
    tall = count // deep
    pairs = owners // 2
    vmem = pl.BlockSpec(memory_space=pltpu.VMEM)
    hbm = pl.BlockSpec(memory_space=pl.ANY)
    bf16, f32 = jnp.bfloat16, jnp.float32
    dma = pltpu.SemaphoreType.DMA
    return pl.pallas_call(
        functools.partial(layer, count, owners, tuple(passes)),
        out_shape=jax.ShapeDtypeStruct((mine, width), bf16),
        in_specs=[hbm, vmem, hbm] + [hbm] * 3 + [vmem] * 10,
        out_specs=vmem,
        scratch_shapes=[
            pltpu.VMEM((count, 2, packed, latent_size), bf16),
            pltpu.VMEM((count * rows, LANES), bf16),
            pltpu.VMEM((3, count * depth, hidden), bf16),
            pltpu.VMEM((owners, rows, sizes[0]), bf16),
            pltpu.VMEM((owners, rows, sizes[1]), bf16),
            pltpu.VMEM((rows, sizes[0]), bf16),
            pltpu.VMEM((rows, sizes[1]), bf16),
            pltpu.VMEM((rows, max(features, hidden)), bf16),
            pltpu.VMEM((features, width), bf16),
            pltpu.VMEM((owners * mine, width), bf16),
            pltpu.VMEM((rows, width), bf16),
            pltpu.VMEM((rows, width), bf16),
            pltpu.VMEM((rows, hidden), f32),
            pltpu.VMEM((2, mine, width), bf16),
            pltpu.VMEM((mine, width), bf16),
            pltpu.VMEM((2, most, 1, rows), f32),
            pltpu.VMEM((2, tallest, rows), f32),
            dma((count,)),
            dma((tall,)),
            dma((tall, deep)),
            dma((count,)),
            dma((3, count)),
            dma((3, 2)),
            dma((3, tall)),
            dma((3, tall, deep)),
            dma((3, count)),
            dma((6,)),
            dma((2, pairs)),
            dma((owners,)),
            dma((2, pairs)),
            dma((2, 2, pairs)),
            dma((2, owners)),
            dma((2, 2, pairs)),
            dma((count, pairs)),
            dma((count, pairs)),
            dma,
            dma,
            dma((2,)),
            dma((2,)),
            pltpu.VMEM((pairs - 1, 2 * mine, width), bf16),
            pltpu.VMEM((counts[0], fulls[0], rows), bf16),
            pltpu.VMEM((counts[1], fulls[1], rows), bf16),
            pltpu.VMEM((latent_size, counts[1] * LANES), bf16),
            pltpu.VMEM((sizes[0], latent_size), bf16),
            pltpu.VMEM((sizes[1], latent_size), bf16),
            pltpu.VMEM((8, LANES), f32),
        ],
        compiler_params=pltpu.CompilerParams(
            collective_id=0, has_side_effects=True, vmem_limit_bytes=67043328
        ),
        cost_estimate=pl.CostEstimate(
            flops=10**11, bytes_accessed=3 * 10**7, transcendentals=2 * 10**7
        ),
    )(
        resid,
        mix_gain,
        out_weight,
        gate_weight,
        up_weight,
        down_weight,
        kv_latent,
        jnp.transpose(rope_key),
        kv_gain,
        turns,
        jnp.transpose(query_large),
        jnp.transpose(query_small),
        up_key_large,
        up_key_small,
        up_value_large,
        up_value_small,
    )


def solution(mesh):
    placed = (
        P(("sp", "tp"), None),
        P("sp", "tp"),
        P("sp", "tp"),
        P("sp", None),
        P("sp", None),
        P(),
        P(None, "tp"),
        P(None, "tp"),
        P(None, "tp"),
        P(None, "tp"),
        P(),
        P(),
        P("sp", "tp"),
        P("sp", "tp"),
        P("sp", "tp"),
    )
    return jax.shard_map(
        functools.partial(on_device, mesh.shape["sp"], mesh.shape["tp"]), mesh=mesh, in_specs=placed, out_specs=P(("sp", "tp"), None), check_vma=False
    )
```
